128 devices in a mesh: sp: 32 (over z, y, core), tp: 4 (over x).
Axes of the slice: x: 4, y: 4, z: 4, core: 2. Of those that a mesh axis runs over, the one named last changes fastest.
Arguments:
- inputs: bfloat16 [49152, 2048], P('sp'), may hold values from -6 to 6
- norm_gain: float32 [2048], replicated, may hold values from 0.1 to 1.9
- pool_weight: bfloat16 [2048, 1024], P(None, 'tp'), may hold values from -0.125 to 0.125
- query_weight: bfloat16 [2048, 1024], P(None, 'tp'), may hold values from -0.125 to 0.125
- forget_weight: bfloat16 [2048, 1024], P(None, 'tp'), may hold values from -0.125 to 0.125
- value_weight: bfloat16 [2048, 1024], P(None, 'tp'), may hold values from -0.125 to 0.125
- outgate_weight: bfloat16 [2048, 1024], P(None, 'tp'), may hold values from -0.125 to 0.125
- pool_mix: bfloat16 [4, 256, 256], P('tp'), may hold values from -0.375 to 0.375
- pool_scale: float32 [1024], P('tp'), may hold values from 0.1 to 1.9
- lower_bound: float32 [1024], P('tp'), may hold values from 0.9 to 1
- extra_decay: float32 [49152, 8], P('sp', 'tp'), may hold values from -1 to 0
- recur_gain: float32 [1024], P('tp'), may hold values from 0.1 to 1.9
- init_state: float32 [8, 128, 128], P('tp'), may hold values from -0.0067658233 to 0.0067658233
- out_pool: bfloat16 [1024, 2048], P('tp'), may hold values from -0.125 to 0.125
- out_recur: bfloat16 [1024, 2048], P('tp'), may hold values from -0.125 to 0.125
Outputs:
- mixed: bfloat16 [49152, 2048], P(('sp', 'tp'))
The draws below stay inside these ranges and needn't reach their ends.
All inputs are finite; a program needn't handle non-finite values.
Results may differ from the reference program's by a relative error of at most 0.014.
Values may be sent and summed in bfloat16 or wider, within the bound.
A program may use at most 128 MiB of HBM per device.

```python
import jax
import jax.numpy as jnp
from jax import lax

D = 2048
BRANCH = 1024
GROUPS = 4
HEAD_K = 128
BLOCK = 64
TOK_DEV = 1536
GROUP_W = 256
HEADS = 8
SEQUENCE_LENGTH = 49152


def draw_lower_bound(key, part):
    count_of_heads = BRANCH // HEAD_K
    key_slow, key_fast, key_pick = jax.random.split(jax.random.fold_in(key, 11), 3)
    slow_gap = jnp.exp(jax.random.uniform(key_slow, (BRANCH,), jnp.float32, jnp.log(0.15), 0.0)) / SEQUENCE_LENGTH
    fast_head = jax.random.bernoulli(key_pick, 0.5, (count_of_heads,))
    fast_gap = jnp.exp(jax.random.uniform(key_fast, (BRANCH,), jnp.float32, jnp.log(0.03), jnp.log(0.08)))
    fast_channel = jnp.repeat(fast_head, HEAD_K)
    gap = jnp.where(fast_channel, fast_gap, slow_gap)
    return (1.0 - gap).astype(jnp.float32)


def draw_extra_decay(key, part):
    count_of_heads = BRANCH // HEAD_K
    key_rate, key_location, key_depth = jax.random.split(jax.random.fold_in(key, 23), 3)
    span_count = SEQUENCE_LENGTH // TOK_DEV
    rate = jnp.exp(jax.random.uniform(key_rate, (span_count, count_of_heads), jnp.float32, jnp.log(0.1), jnp.log(0.6)))
    base_offset = -jnp.repeat(rate, TOK_DEV, axis=0) / SEQUENCE_LENGTH
    spurt_rows = jax.random.randint(key_location, (2, count_of_heads), 0, SEQUENCE_LENGTH)
    layer_depth = jnp.log(jax.random.uniform(key_depth, (2, count_of_heads), jnp.float32, 0.55, 0.8))
    token_positions = jnp.arange(SEQUENCE_LENGTH, dtype=jnp.int32)[:, None, None]
    spurt_list = jnp.sum(jnp.where(token_positions == spurt_rows[None], layer_depth[None], 0.0), axis=1)
    return (base_offset + spurt_list).astype(jnp.float32)


def steps_of(rng, extent, cuts, low, high):
    level, own = 1.0, jax.random.fold_in(rng, 6)
    for position, shards_of in cuts:
        draws = jnp.exp(jax.random.uniform(jax.random.fold_in(own, position), (shards_of,), jnp.float32, low / len(cuts), high / len(cuts)))
        level = level * jnp.repeat(draws, extent[position] // shards_of).reshape([-1 if axis == position else 1 for axis in range(len(extent))])
    return level


def noise(own_key, shape, deviation, limit, cuts=(), kind=jnp.bfloat16):
    drawn = jax.random.normal(own_key, shape, jnp.float32) * deviation
    if len(cuts) > 0:
        drawn = steps_of(own_key, shape, cuts, -0.22, 0.18) * drawn
    return jnp.clip(drawn, min=-limit, max=limit).astype(kind)


def setup_inputs(seed: int = 0) -> dict:
    splits = jax.random.split(jax.random.key(seed), 16)
    inputs = noise(splits[0], (SEQUENCE_LENGTH, D), 1.0, 6.0, ((0, 32),))
    norm_gain = jnp.clip(1.0 + 0.18 * jax.random.normal(splits[1], (D,), jnp.float32), 0.1, 1.9)
    pool_weight = noise(splits[2], (D, BRANCH), D ** -0.5, 0.125, ((1, 4),))
    query_weight = noise(splits[3], (D, BRANCH), D ** -0.5, 0.125, ((1, 4),))
    forget_weight = noise(splits[4], (D, BRANCH), D ** -0.5, 0.125, ((1, 4),))
    value_weight = noise(splits[5], (D, BRANCH), D ** -0.5, 0.125, ((1, 4),))
    outgate_weight = noise(splits[6], (D, BRANCH), D ** -0.5, 0.125, ((1, 4),))
    pool_mix = noise(splits[7], (GROUPS, GROUP_W, GROUP_W), GROUP_W ** -0.5, 0.375, ((0, 4),))
    pool_scale = jnp.clip(1.0 + 0.18 * jax.random.normal(splits[8], (BRANCH,), jnp.float32), 0.1, 1.9)
    lower_bound = draw_lower_bound(jax.random.fold_in(splits[15], 71), 0)
    extra_decay = draw_extra_decay(jax.random.fold_in(splits[15], 71), 0)
    recur_gain = jnp.clip(1.0 + 0.18 * jax.random.normal(splits[11], (BRANCH,), jnp.float32), 0.1, 1.9)
    init_state = noise(splits[12], (HEADS, HEAD_K, HEAD_K), (0.25 * SEQUENCE_LENGTH ** -0.5), 0.0067658233, ((0, 4),), jnp.float32)
    out_pool = noise(splits[13], (BRANCH, D), (2 * BRANCH) ** -0.5, 0.125, ((0, 4),))
    out_recur = noise(splits[14], (BRANCH, D), (2 * BRANCH) ** -0.5, 0.125, ((0, 4),))
    return dict(inputs=inputs, norm_gain=norm_gain, pool_weight=pool_weight, query_weight=query_weight, forget_weight=forget_weight, value_weight=value_weight, outgate_weight=outgate_weight, pool_mix=pool_mix, pool_scale=pool_scale, lower_bound=lower_bound, extra_decay=extra_decay, recur_gain=recur_gain, init_state=init_state, out_pool=out_pool, out_recur=out_recur)


norm_eps = 1e-05
top_precision = lax.Precision.HIGHEST

def norm_rows(array, scale_vec):
    widened = array.astype(jnp.float32)
    scaled = widened * lax.rsqrt(lax.optimization_barrier(jnp.mean(widened * widened, axis=-1, keepdims=True)) + norm_eps)
    return (scaled * scale_vec).astype(jnp.bfloat16)

def window_sums(widened):
    results = []
    current = widened
    for level_idx in range(GROUPS):
        stride = 2 ** level_idx
        shifted = jnp.pad(current, ((stride, 0), (0, 0)))[:current.shape[0]]
        current = current + shifted
        results.append(current)
    return results

def pool_branch(pool_in, pool_mix, pool_scale):
    row_count = pool_in.shape[0]
    group_width = pool_mix.shape[1]
    widened = pool_in.astype(jnp.float32)
    window_totals = window_sums(widened)
    token_positions = jnp.arange(row_count, dtype=jnp.int32)
    pieces = []
    for group_idx in range(pool_mix.shape[0]):
        columns = slice(group_idx * group_width, (group_idx + 1) * group_width)
        reach = jnp.minimum(token_positions + 1, 2 ** (group_idx + 1)).astype(jnp.float32)
        pieces.append(window_totals[group_idx][:, columns] / reach[:, None] - widened[:, columns])
    pooled = jnp.stack(pieces, axis=1).astype(jnp.bfloat16)
    mixed_groups = jnp.einsum('rgc,gcd->rgd', pooled.astype(jnp.float32), pool_mix.astype(jnp.float32))
    return (mixed_groups.reshape(row_count, -1) * pool_scale).astype(jnp.bfloat16)

def recur_inputs(query_raw, forget_raw, value_raw, bound_vec, extra_log, head_k, block_len):
    row_count = query_raw.shape[0]
    count_of_heads = query_raw.shape[1] // head_k
    block_count = row_count // block_len
    forget_pre = forget_raw.astype(jnp.float32)
    log_f = jnp.logaddexp(jnp.log(bound_vec), jnp.log1p(-bound_vec) + jax.nn.log_sigmoid(forget_pre))
    log_f = log_f.reshape(row_count, count_of_heads, head_k) + extra_log[:, :, None]
    key_input = ((1.0 - bound_vec) * jax.nn.sigmoid(-forget_pre)).reshape(row_count, count_of_heads, head_k)
    query_input = jax.nn.silu(query_raw.astype(jnp.float32)).reshape(row_count, count_of_heads, head_k)
    value_input = value_raw.astype(jnp.float32).reshape(row_count, count_of_heads, head_k)

    def to_blocks(array):
        return array.reshape(block_count, block_len, count_of_heads, head_k).transpose(2, 0, 1, 3)
    return (to_blocks(query_input), to_blocks(key_input), to_blocks(value_input), to_blocks(log_f))

def block_parts(query_input, key_input, value_input, log_f):
    block_len = log_f.shape[2]
    cum_log = jnp.cumsum(log_f, axis=2)
    last_log = cum_log[:, :, -1:, :]
    query_dec = query_input * jnp.exp(cum_log)
    key_dec = key_input * jnp.exp(-cum_log)
    scores = jnp.einsum('hntk,hnsk->hnts', query_dec, key_dec, precision=top_precision)
    causal = jnp.tril(jnp.ones((block_len, block_len), dtype=bool))
    scores = jnp.where(causal, scores, 0.0)
    within = jnp.einsum('hnts,hnsv->hntv', scores, value_input, precision=top_precision)
    contrib = jnp.einsum('hnsk,hnsv->hnkv', key_input * jnp.exp(last_log - cum_log), value_input, precision=top_precision)
    decays = jnp.exp(last_log[:, :, 0, :])
    return (query_dec, within, decays, contrib)

def chain(earlier, later_part):
    return (earlier[0] * later_part[0], later_part[0][..., None] * earlier[1] + later_part[1])

def recur_branch(query_raw, forget_raw, value_raw, outgate_raw, bound_vec, extra_log, recur_gain, init_state):
    row_count = query_raw.shape[0]
    head_k = init_state.shape[1]
    count_of_heads = init_state.shape[0]
    query_in, key_in, value_in, log_f = recur_inputs(query_raw, forget_raw, value_raw, bound_vec, extra_log, head_k, BLOCK)
    query_dec, within, decays, contrib = block_parts(query_in, key_in, value_in, log_f)
    running = lax.associative_scan(chain, (decays, contrib), axis=1)
    enter_a = jnp.concatenate([jnp.ones_like(decays[:, :1]), running[0][:, :-1]], axis=1)
    enter_s = jnp.concatenate([jnp.zeros_like(contrib[:, :1]), running[1][:, :-1]], axis=1)
    state_in = enter_s + enter_a[..., None] * init_state[:, None]
    recur_out = within + jnp.einsum('hntk,hnkv->hntv', query_dec, state_in, precision=top_precision)
    recur_out = recur_out.transpose(1, 2, 0, 3).reshape(row_count, count_of_heads, head_k)
    recur_out = recur_out * lax.rsqrt(lax.optimization_barrier(jnp.mean(recur_out * recur_out, axis=-1, keepdims=True)) + norm_eps)
    recur_out = recur_out * recur_gain.reshape(count_of_heads, head_k)
    gated = recur_out.reshape(row_count, count_of_heads * head_k) * jax.nn.silu(outgate_raw.astype(jnp.float32))
    return gated.astype(jnp.bfloat16)

def reference(inputs, norm_gain, pool_weight, query_weight, forget_weight, value_weight, outgate_weight, pool_mix, pool_scale, lower_bound, extra_decay, recur_gain, init_state, out_pool, out_recur):
    normed = norm_rows(inputs, norm_gain)
    pool_in = jnp.dot(normed, pool_weight, preferred_element_type=jnp.float32).astype(jnp.bfloat16)
    query_raw = jnp.dot(normed, query_weight, preferred_element_type=jnp.float32).astype(jnp.bfloat16)
    forget_raw = jnp.dot(normed, forget_weight, preferred_element_type=jnp.float32).astype(jnp.bfloat16)
    value_raw = jnp.dot(normed, value_weight, preferred_element_type=jnp.float32).astype(jnp.bfloat16)
    outgate_raw = jnp.dot(normed, outgate_weight, preferred_element_type=jnp.float32).astype(jnp.bfloat16)
    y_pool = pool_branch(pool_in, pool_mix, pool_scale)
    y_recur = recur_branch(query_raw, forget_raw, value_raw, outgate_raw, lower_bound, extra_decay, recur_gain, init_state)
    summed = jnp.dot(y_pool, out_pool, preferred_element_type=jnp.float32)
    summed = summed + jnp.dot(y_recur, out_recur, preferred_element_type=jnp.float32)
    return summed.astype(jnp.bfloat16)
```

```python
import functools

import jax
import jax.numpy as jnp
from jax import lax
from jax.experimental import pallas as pl
from jax.experimental.pallas import tpu as pltpu
from jax.sharding import PartitionSpec as P

MESH = pl.DeviceIdType.MESH
F32 = jnp.float32
BF16 = jnp.bfloat16
EPS = 1e-5

ROWS = 1536
CH = 256
NCH = ROWS // CH
BL = 128
NB = ROWS // BL
C = 256
HK = 128
D = 2048
OUT = 384

NT = (((1,), (1,)), ((), ()))
TN = (((0,), (0,)), ((), ()))
NN = (((1,), (0,)), ((), ()))


def dot(a, b, dims=NN):
    return lax.dot_general(a, b, dims, preferred_element_type=F32)


def half_tanh_sigmoid(v):
    return 0.5 + 0.5 * jnp.tanh(0.5 * v)


def log1p_neg(k):
    s = jnp.full_like(k, 1.0 / 8)
    for n in (7, 6, 5, 4, 3, 2):
        s = s * k + 1.0 / n
    return -(k + (k * k) * s)


def kernel(
    x_hbm, gain_hbm, wp_hbm, wq_hbm, wf_hbm, wv_hbm, wg_hbm, mix_hbm, pscale_hbm, lb_hbm,
    extra_hbm, rgain_hbm, init_hbm, op_hbm, or_hbm,
    out_ref,
    xbuf, nbuf, wfv, wqgp, wout, gain, pscale, lb, rgain, extra, mix, init,
    fbuf, vbuf, ebuf, kbuf, qbuf, winbuf, gbuf, pbuf, sloc, run, lrun, vecs,
    totsend, totrecv, ybuf, zbuf, pst, carr, tril, band,
    ypbuf, ypseen, yrbuf, yrseen, acc,
    lsem, w1s, w1r, w2s, w2r, w3s, w3r, es, er, ys, yr_, zs, zr, ps_, pr_, hs, hr, aps, apr, ars, arr,
):
    x = lax.axis_index("tp")
    sp = lax.axis_index("sp")
    c = lax.rem(sp, 2)
    y = lax.rem(lax.div(sp, 2), 4)
    z = lax.div(sp, 8)

    def dev(spi, tpi):
        return {"sp": spi, "tp": tpi}

    def xpeer(k):
        return dev(sp, lax.rem(x + k, 4))

    def ypeer(k):
        return dev(z * 8 + lax.rem(y + k, 4) * 2 + c, x)

    def zpeer(k):
        return dev(lax.rem(z + k, 4) * 8 + y * 2 + c, x)

    sib = dev(sp + 1 - 2 * c, x)
    nxt = dev(lax.rem(sp + 1, 32), x)
    prv = dev(lax.rem(sp + 31, 32), x)

    count = [0]

    def load(src, dst):
        i = count[0]
        count[0] += 1
        cp = pltpu.make_async_copy(src, dst, lsem.at[i])
        cp.start()
        return cp

    def remote(src, dst, ssem, rsem, to):
        cp = pltpu.make_async_remote_copy(
            src_ref=src, dst_ref=dst, send_sem=ssem, recv_sem=rsem, device_id=to, device_id_type=MESH
        )
        return cp

    def rows(i, n):
        return pl.ds(pl.multiple_of(i * n, n), n)

    bar = pltpu.get_barrier_semaphore()
    for k in (1, 2, 3):
        for peer in (xpeer, ypeer, zpeer):
            pl.semaphore_signal(bar, inc=1, device_id=peer(k), device_id_type=MESH)
    for to in (sib, nxt, prv):
        pl.semaphore_signal(bar, inc=1, device_id=to, device_id_type=MESH)

    l_gain = load(gain_hbm, gain)
    l_x = [load(x_hbm.at[pl.ds(0, CH)], xbuf.at[pl.ds(0, CH)])]
    l_wf = load(wf_hbm, wfv.at[:, pl.ds(0, C)])
    l_wv = load(wv_hbm, wfv.at[:, pl.ds(C, C)])
    l_lb = load(lb_hbm, lb)
    l_extra = load(extra_hbm, extra)
    l_x.append(load(x_hbm.at[pl.ds(CH, CH)], xbuf.at[pl.ds(CH, CH)]))
    l_op = load(op_hbm, wout.at[0, rows(x, 256)])
    l_or = load(or_hbm, wout.at[1, rows(x, 256)])
    for i in range(2, NCH):
        l_x.append(load(x_hbm.at[pl.ds(i * CH, CH)], xbuf.at[pl.ds(i * CH, CH)]))
    l_q = load(wq_hbm, wqgp.at[:, pl.ds(0, C)])
    l_g = load(wg_hbm, wqgp.at[:, pl.ds(C, C)])
    l_p = load(wp_hbm, wqgp.at[:, pl.ds(2 * C, C)])
    l_init = load(init_hbm, init)
    l_rg = load(rgain_hbm, rgain)
    l_ps = load(pscale_hbm, pscale)
    l_mix = load(mix_hbm, mix)

    r_i = lax.broadcasted_iota(jnp.int32, (BL, BL), 0)
    c_i = lax.broadcasted_iota(jnp.int32, (BL, BL), 1)
    tril[...] = (c_i <= r_i).astype(F32)
    w = lax.shift_left(jnp.int32(2), x)
    r_w = lax.broadcasted_iota(jnp.int32, (BL, 2 * BL), 0)
    c_w = lax.broadcasted_iota(jnp.int32, (BL, 2 * BL), 1)
    diff = r_w + BL - c_w
    band[...] = jnp.where((diff >= 0) & (diff < w), 1.0, 0.0).astype(BF16)

    def norm(i):
        r = pl.ds(i * CH, CH)
        v = xbuf[r, :].astype(F32)
        rs = lax.rsqrt(jnp.sum(v * v, axis=-1, keepdims=True) * (1.0 / D) + EPS)
        nbuf[r, :] = (v * rs * gain[...]).astype(BF16)

    def proj_fv(i):
        r = pl.ds(i * CH, CH)
        o = dot(nbuf[r, :], wfv[...])
        fbuf[r, :] = o[:, :C]
        vbuf[r, :] = o[:, C:].astype(BF16)

    def state_block(b):
        r = pl.ds(b * BL, BL)
        f = fbuf[r, :]
        key = (1.0 - lb[...]) / (1.0 + jnp.exp(f))
        lf = log1p_neg(key)
        hi = lf.astype(BF16)
        lo = (lf - hi.astype(F32)).astype(BF16)
        t = tril[...]
        tb = t.astype(BF16)
        ones = jnp.ones((2 * BL, HK), BF16)
        cums = []
        for h in range(2):
            hc = slice(h * HK, (h + 1) * HK)
            te = t * extra[h : h + 1, b * BL : (b + 1) * BL]
            te_hi = te.astype(BF16)
            te_lo = (te - te_hi.astype(F32)).astype(BF16)
            lhs = jnp.concatenate([tb, tb, te_hi, te_lo], axis=1)
            rhs = jnp.concatenate([hi[:, hc], lo[:, hc], ones], axis=0)
            cums.append(dot(lhs, rhs))
        cum = jnp.concatenate(cums, axis=1)
        m = cum[BL // 2 - 1 : BL // 2, :]
        last = cum[BL - 1 : BL, :]
        rel = cum - m
        ebuf[r, :] = jnp.exp(rel)
        kd = key * jnp.exp(-rel)
        kbuf[r, :] = kd.astype(BF16)
        kst = (kd * jnp.exp(last - m)).astype(BF16)
        lpre = lrun[...]
        vecs[b, 0:1, :] = lpre
        vecs[b, 1:2, :] = m
        lrun[...] = lpre + last
        a = jnp.exp(last)
        v = vbuf[r, :]
        for h in range(2):
            hc = slice(h * HK, (h + 1) * HK)
            contrib = dot(v[:, hc], kst[:, hc], TN)
            s = run[h]
            sloc[b, h] = s
            run[h] = s * a[:, hc] + contrib

    def proj_qgp(i):
        r = pl.ds(i * CH, CH)
        o = dot(nbuf[r, :], wqgp[...])
        q = o[:, :C]
        qbuf[r, :] = (q * half_tanh_sigmoid(q) * ebuf[r, :]).astype(BF16)
        g = o[:, C : 2 * C]
        gbuf[r, :] = g * half_tanh_sigmoid(g) * rgain[...]
        pbuf[pl.ds(BL + i * CH, CH), :] = o[:, 2 * C :].astype(BF16)

    def score_block(b):
        r = pl.ds(b * BL, BL)
        causal = tril[...] > 0.5
        for h in range(2):
            hc = slice(h * HK, (h + 1) * HK)
            s = dot(qbuf[r, hc], kbuf[r, hc], NT)
            s = jnp.where(causal, s, 0.0).astype(BF16)
            winbuf[r, hc] = dot(s, vbuf[r, hc])

    def pool_block(b):
        ext = pbuf[pl.ds(pl.multiple_of(b * BL, BL), 2 * BL), :]
        sums = dot(band[...], ext)
        t = sp * ROWS + b * BL + lax.broadcasted_iota(jnp.int32, (BL, 1), 0)
        cnt = jnp.minimum(t + 1, w).astype(F32)
        pooled = (sums / cnt - ext[BL:, :].astype(F32)).astype(BF16)
        return (dot(pooled, mix[0]) * pscale[...]).astype(BF16)

    def out_block(b):
        r = pl.ds(pl.multiple_of(b * BL, BL), BL)
        lpre = vecs[b, 0:1, :]
        m = vecs[b, 1:2, :]
        em = jnp.exp(m)
        elm = jnp.exp(lpre + m)
        parts = []
        for h in range(2):
            hc = slice(h * HK, (h + 1) * HK)
            st = (sloc[b, h] * em[:, hc] + carr[h] * elm[:, hc]).astype(BF16)
            o = winbuf[r, hc] + dot(qbuf[r, hc], st, NT)
            ms = jnp.sum(o * o, axis=-1, keepdims=True) * (1.0 / HK)
            parts.append(o * lax.rsqrt(ms + EPS) * gbuf[r, hc])
        return jnp.concatenate(parts, axis=1).astype(BF16)

    l_gain.wait()
    l_x[0].wait()
    norm(0)
    l_wf.wait()
    l_wv.wait()
    l_lb.wait()
    l_extra.wait()
    run[...] = jnp.zeros_like(run)
    lrun[...] = jnp.zeros_like(lrun)
    pbuf[pl.ds(0, BL - 16), :] = jnp.zeros((BL - 16, C), BF16)

    l_op.wait()
    l_or.wait()
    pl.semaphore_wait(bar, 12)
    pa = x * 256 + y * 32
    pb = x * 256 + 128 + z * 32
    w1 = []
    for k in (2, 1, 3):
        for a, at in enumerate((pa, pb)):
            sl = wout.at[c, pl.ds(pl.multiple_of(at, 32), 32)]
            cp = remote(sl, sl, w1s.at[k - 1, a], w1r.at[k - 1, a], xpeer(k))
            cp.start()
            w1.append(cp)

    for i in range(NCH):
        if i + 1 < NCH:
            l_x[i + 1].wait()
        proj_fv(i)
        if i + 1 < NCH:
            norm(i + 1)
        if i > 0:
            state_block(2 * i - 2)
            state_block(2 * i - 1)
    state_block(NB - 2)
    state_block(NB - 1)

    for h in range(2):
        totsend[h, 0:HK, :] = run[h]
        al = jnp.exp(lrun[:, h * HK : (h + 1) * HK])
        totsend[h, HK : HK + 8, :] = jnp.broadcast_to(al, (8, HK))
    e_cp = remote(totsend, totrecv, es, er, sib)
    e_cp.start()
    l_q.wait()
    l_g.wait()
    l_p.wait()
    l_rg.wait()

    def chain(ea, eS, la, lS):
        return ea * la, la * eS + lS

    order = (5, 0, 1, 2, 3, 4)
    pending = {}
    for n, i in enumerate(order):
        proj_qgp(i)
        if n > 0:
            j = order[n - 1]
            score_block(2 * j)
            score_block(2 * j + 1)
        if n == 0:
            h_cp = remote(
                pbuf.at[pl.ds(BL + ROWS - 16, 16)], pbuf.at[pl.ds(BL - 16, 16)], hs, hr, nxt
            )
            h_cp.start()
            e_cp.wait()
            oS, oa = totsend[c, 0:HK, :], totsend[c, HK : HK + 1, :]
            sS, sa = totrecv[c, 0:HK, :], totrecv[c, HK : HK + 1, :]
            first = c == 0
            ea, eS = jnp.where(first, oa, sa), jnp.where(first, oS, sS)
            la, lS = jnp.where(first, sa, oa), jnp.where(first, sS, oS)
            ta, tS = chain(ea, eS, la, lS)
            ybuf[y, 0:HK, :] = tS
            ybuf[y, HK : HK + 8, :] = jnp.broadcast_to(ta, (8, HK))
            y_cp = []
            for k in (2, 1, 3):
                cp = remote(ybuf.at[y], ybuf.at[y], ys.at[k - 1], yr_.at[k - 1], ypeer(k))
                cp.start()
                y_cp.append(cp)
        if n == 2:
            for cp in y_cp:
                cp.wait()
            ta = jnp.ones((1, HK), F32)
            tS = jnp.zeros((HK, HK), F32)
            ya, yS = ta, tS
            for j in range(4):
                ta, tS = chain(ta, tS, ybuf[j, HK : HK + 1, :], ybuf[j, 0:HK, :])
                ya = jnp.where(y > j, ta, ya)
                yS = jnp.where(y > j, tS, yS)
            zbuf[z, 0:HK, :] = tS
            zbuf[z, HK : HK + 8, :] = jnp.broadcast_to(ta, (8, HK))
            pst[0:HK, :] = yS
            pst[HK : HK + 8, :] = jnp.broadcast_to(ya, (8, HK))
            z_cp = []
            for k in (2, 1, 3):
                cp = remote(zbuf.at[z], zbuf.at[z], zs.at[k - 1], zr.at[k - 1], zpeer(k))
                cp.start()
                z_cp.append(cp)
            for cp in w1:
                cp.wait()
            w2 = []
            for k in (2, 1, 3):
                j = lax.rem(x + 4 - k, 4)
                sl = wout.at[c, pl.ds(pl.multiple_of(j * 256 + y * 32, 32), 32)]
                for q in (2, 1, 3):
                    cp = remote(sl, sl, w2s.at[0, k - 1, q - 1], w2r.at[0, k - 1, q - 1], ypeer(q))
                    cp.start()
                    w2.append(cp)
        if n == 4:
            for cp in z_cp:
                cp.wait()
            ta = jnp.ones((1, HK), F32)
            tS = jnp.zeros((HK, HK), F32)
            za, zS = ta, tS
            for j in range(4):
                ta, tS = chain(ta, tS, zbuf[j, HK : HK + 1, :], zbuf[j, 0:HK, :])
                za = jnp.where(z > j, ta, za)
                zS = jnp.where(z > j, tS, zS)
            l_init.wait()
            pa_, pS_ = chain(za, zS, pst[HK : HK + 1, :], pst[0:HK, :])
            carr[c] = pa_ * jnp.transpose(init[c]) + pS_
            p_cp = remote(carr.at[c], carr.at[c], ps_, pr_, sib)
            p_cp.start()
            for k in (2, 1, 3):
                j = lax.rem(x + 4 - k, 4)
                sl = wout.at[c, pl.ds(pl.multiple_of(j * 256 + 128 + z * 32, 32), 32)]
                for q in (2, 1, 3):
                    cp = remote(sl, sl, w2s.at[1, k - 1, q - 1], w2r.at[1, k - 1, q - 1], zpeer(q))
                    cp.start()
                    w2.append(cp)
    score_block(2 * order[-1])
    score_block(2 * order[-1] + 1)

    l_ps.wait()
    l_mix.wait()
    h_cp.wait()

    @pl.when(sp == 0)
    def _():
        pbuf[pl.ds(BL - 16, 16), :] = jnp.zeros((16, C), BF16)

    ap = []
    for k in (2, 1, 3, 0):
        d = lax.rem(x + k, 4)
        for s in range(3):
            blk = pool_block(d * 3 + s)
            if k == 0:
                ypseen[x, pl.ds(s * BL, BL), :] = blk
            else:
                ypbuf[k - 1, pl.ds(s * BL, BL), :] = blk
        if k:
            cp = remote(ypbuf.at[k - 1], ypseen.at[x], aps.at[k - 1], apr.at[k - 1], xpeer(k))
            cp.start()
            ap.append(cp)

    p_cp.wait()
    for h in range(2):
        pcur = carr[h]
        later = totrecv[h, HK : HK + 1, :] * pcur + totrecv[h, 0:HK, :]
        carr[h] = jnp.where(c == 0, pcur, later)
    ar = []
    for k in (2, 1, 3, 0):
        d = lax.rem(x + k, 4)
        for s in range(3):
            blk = out_block(d * 3 + s)
            if k == 0:
                yrseen[x, pl.ds(s * BL, BL), :] = blk
            else:
                yrbuf[k - 1, pl.ds(s * BL, BL), :] = blk
        if k:
            cp = remote(yrbuf.at[k - 1], yrseen.at[x], ars.at[k - 1], arr.at[k - 1], xpeer(k))
            cp.start()
            ar.append(cp)

    for cp in w2:
        cp.wait()
    w3 = []
    for k in (1, 2, 3):
        j = lax.rem(x + 4 - k, 4)
        sl = wout.at[c, rows(j, 256)]
        cp = remote(sl, sl, w3s.at[k - 1], w3r.at[k - 1], sib)
        cp.start()
        w3.append(cp)
    for cp in w3:
        cp.wait()
    for cp in ap:
        cp.wait()
    yp = jnp.concatenate([ypseen[j] for j in range(4)], axis=1)
    for n in range(4):
        nc = pl.ds(n * 512, 512)
        acc[:, nc] = dot(yp, wout[0, :, nc])
    for cp in ar:
        cp.wait()
    yr = jnp.concatenate([yrseen[j] for j in range(4)], axis=1)
    for n in range(4):
        nc = pl.ds(n * 512, 512)
        out_ref[:, nc] = (acc[:, nc] + dot(yr, wout[1, :, nc])).astype(BF16)


def scratch():
    V = pltpu.VMEM
    S = pltpu.SemaphoreType.DMA
    return [
        V((ROWS, D), BF16), V((ROWS, D), BF16), V((D, 2 * C), BF16), V((D, 3 * C), BF16),
        V((2, 4 * C, D), BF16), V((1, D), F32), V((1, C), F32), V((1, C), F32), V((1, C), F32),
        V((2, ROWS), F32), V((1, C, C), BF16), V((2, HK, HK), F32),
        V((ROWS, C), F32), V((ROWS, C), BF16), V((ROWS, C), F32), V((ROWS, C), BF16),
        V((ROWS, C), BF16), V((ROWS, C), F32), V((ROWS, C), F32), V((BL + ROWS, C), BF16),
        V((NB, 2, HK, HK), F32), V((2, HK, HK), F32), V((1, C), F32), V((NB, 2, C), F32),
        V((2, HK + 8, HK), F32), V((2, HK + 8, HK), F32), V((4, HK + 8, HK), F32), V((4, HK + 8, HK), F32),
        V((HK + 8, HK), F32), V((2, HK, HK), F32), V((BL, BL), F32), V((BL, 2 * BL), BF16),
        V((3, OUT, C), BF16), V((4, OUT, C), BF16), V((3, OUT, C), BF16), V((4, OUT, C), BF16),
        V((OUT, D), F32),
        S((20,)), S((3, 2)), S((3, 2)), S((2, 3, 3)), S((2, 3, 3)), S((3,)), S((3,)),
        S(()), S(()), S((3,)), S((3,)), S((3,)), S((3,)), S(()), S(()), S(()), S(()),
        S((3,)), S((3,)), S((3,)), S((3,)),
    ]


def per_device(
    inputs, norm_gain, pool_weight, query_weight, forget_weight, value_weight, outgate_weight,
    pool_mix, pool_scale, lower_bound, extra_decay, recur_gain, init_state, out_pool, out_recur,
):
    anyspec = pl.BlockSpec(memory_space=pl.ANY)
    return pl.pallas_call(
        kernel,
        out_shape=jax.ShapeDtypeStruct((OUT, D), BF16),
        in_specs=[anyspec] * 15,
        out_specs=pl.BlockSpec(memory_space=pltpu.VMEM),
        scratch_shapes=scratch(),
        compiler_params=pltpu.CompilerParams(
            collective_id=0, has_side_effects=True, vmem_limit_bytes=63 * 1024 * 1024
        ),
    )(
        inputs, norm_gain.reshape(1, D), pool_weight, query_weight, forget_weight, value_weight,
        outgate_weight, pool_mix, pool_scale.reshape(1, C), lower_bound.reshape(1, C),
        extra_decay.T, recur_gain.reshape(1, C), init_state, out_pool, out_recur,
    )


def solution(mesh):
    placed = (
        P("sp", None), P(), P(None, "tp"), P(None, "tp"), P(None, "tp"), P(None, "tp"), P(None, "tp"),
        P("tp", None, None), P("tp"), P("tp"), P("sp", "tp"), P("tp"), P("tp", None, None),
        P("tp", None), P("tp", None),
    )
    return jax.shard_map(
        per_device, mesh=mesh, in_specs=placed, out_specs=P(("sp", "tp"), None), check_vma=False
    )
```

```python
import functools

import jax
import jax.numpy as jnp
from jax import lax
from jax.experimental import pallas as pl
from jax.experimental.pallas import tpu as pltpu
from jax.sharding import PartitionSpec as P

MESH = pl.DeviceIdType.MESH
F32 = jnp.float32
BF16 = jnp.bfloat16
EPS = 1e-5

ROWS = 1536
CH = 256
NCH = ROWS // CH
BL = 128
NB = ROWS // BL
C = 256
HK = 128
D = 2048
OUT = 384

NT = (((1,), (1,)), ((), ()))
TN = (((0,), (0,)), ((), ()))
NN = (((1,), (0,)), ((), ()))


def dot(a, b, dims=NN):
    return lax.dot_general(a, b, dims, preferred_element_type=F32)


def half_tanh_sigmoid(v):
    return 0.5 + 0.5 * jnp.tanh(0.5 * v)


def log1p_neg(k):
    s = jnp.full_like(k, 1.0 / 8)
    for n in (7, 6, 5, 4, 3, 2):
        s = s * k + 1.0 / n
    return -(k + (k * k) * s)


def kernel(
    x_hbm, gain_hbm, wp_hbm, wq_hbm, wf_hbm, wv_hbm, wg_hbm, mix_hbm, pscale_hbm, lb_hbm,
    extra_hbm, rgain_hbm, init_hbm, op_hbm, or_hbm,
    out_ref,
    xbuf, nbuf, wfv, wqg, wp, wst, wout, gain, pscale, lb, rgain, extra, mix, init,
    fbuf, vbuf, ebuf, kbuf, qbuf, winbuf, gbuf, pbuf, sloc, run, lrun, vecs,
    totsend, totrecv, ybuf, zbuf, pst, carr, tril, band,
    ypbuf, ypseen, yrbuf, yrseen, acc,
    lsem, w1s, w1r, w2s, w2r, w3s, w3r, es, er, ys, yr_, zs, zr, ps_, pr_, hs, hr, aps, apr, ars, arr,
):
    x = lax.axis_index("tp")
    sp = lax.axis_index("sp")
    c = lax.rem(sp, 2)
    y = lax.rem(lax.div(sp, 2), 4)
    z = lax.div(sp, 8)

    def dev(spi, tpi):
        return {"sp": spi, "tp": tpi}

    def xpeer(k):
        return dev(sp, lax.rem(x + k, 4))

    def ypeer(k):
        return dev(z * 8 + lax.rem(y + k, 4) * 2 + c, x)

    def zpeer(k):
        return dev(lax.rem(z + k, 4) * 8 + y * 2 + c, x)

    sib = dev(sp + 1 - 2 * c, x)
    nxt = dev(lax.rem(sp + 1, 32), x)
    prv = dev(lax.rem(sp + 31, 32), x)

    count = [0]

    def load(src, dst):
        i = count[0]
        count[0] += 1
        cp = pltpu.make_async_copy(src, dst, lsem.at[i])
        cp.start()
        return cp

    def remote(src, dst, ssem, rsem, to):
        cp = pltpu.make_async_remote_copy(
            src_ref=src, dst_ref=dst, send_sem=ssem, recv_sem=rsem, device_id=to, device_id_type=MESH
        )
        cp.start()
        return cp

    def rows(i, n):
        return pl.ds(pl.multiple_of(i * n, n), n)

    bar = pltpu.get_barrier_semaphore()
    for k in (1, 2, 3):
        for peer in (xpeer, ypeer, zpeer):
            pl.semaphore_signal(bar, inc=1, device_id=peer(k), device_id_type=MESH)
    for to in (sib, nxt, prv):
        pl.semaphore_signal(bar, inc=1, device_id=to, device_id_type=MESH)

    pa = pl.multiple_of(y * 32, 32)
    pb = pl.multiple_of(128 + z * 32, 32)
    l_gain = load(gain_hbm, gain)
    l_x = [load(x_hbm.at[pl.ds(0, CH)], xbuf.at[pl.ds(0, CH)])]
    l_wf = load(wf_hbm, wfv.at[:, pl.ds(0, C)])
    l_wv = load(wv_hbm, wfv.at[:, pl.ds(C, C)])
    l_lb = load(lb_hbm, lb)
    l_extra = load(extra_hbm, extra)
    l_pc = [load(op_hbm.at[pl.ds(pa, 32)], wst.at[0, 0]), load(op_hbm.at[pl.ds(pb, 32)], wst.at[0, 1])]
    l_pc += [load(or_hbm.at[pl.ds(pa, 32)], wst.at[1, 0]), load(or_hbm.at[pl.ds(pb, 32)], wst.at[1, 1])]
    for i in range(1, NCH):
        l_x.append(load(x_hbm.at[pl.ds(i * CH, CH)], xbuf.at[pl.ds(i * CH, CH)]))
    l_p = load(wp_hbm, wp)
    l_q = load(wq_hbm, wqg.at[:, pl.ds(0, C)])
    l_g = load(wg_hbm, wqg.at[:, pl.ds(C, C)])
    l_init = load(init_hbm, init)
    l_rg = load(rgain_hbm, rgain)
    l_ps = load(pscale_hbm, pscale)
    l_mix = load(mix_hbm, mix)
    l_op = load(op_hbm, wout.at[0, rows(x, 256)])
    l_or = load(or_hbm, wout.at[1, rows(x, 256)])

    r_i = lax.broadcasted_iota(jnp.int32, (BL, BL), 0)
    c_i = lax.broadcasted_iota(jnp.int32, (BL, BL), 1)
    tril[...] = (c_i <= r_i).astype(F32)
    w = lax.shift_left(jnp.int32(2), x)
    r_w = lax.broadcasted_iota(jnp.int32, (BL, 2 * BL), 0)
    c_w = lax.broadcasted_iota(jnp.int32, (BL, 2 * BL), 1)
    diff = r_w + BL - c_w
    band[...] = jnp.where((diff >= 0) & (diff < w), 1.0, 0.0).astype(BF16)

    def norm(i):
        r = pl.ds(i * CH, CH)
        v = xbuf[r, :].astype(F32)
        rs = lax.rsqrt(jnp.sum(v * v, axis=-1, keepdims=True) * (1.0 / D) + EPS)
        nbuf[r, :] = (v * rs * gain[...]).astype(BF16)

    def proj_fv(i):
        r = pl.ds(i * CH, CH)
        o = dot(nbuf[r, :], wfv[...])
        fbuf[r, :] = o[:, :C]
        vbuf[r, :] = o[:, C:].astype(BF16)

    def state_block(b):
        r = pl.ds(b * BL, BL)
        f = fbuf[r, :]
        key = (1.0 - lb[...]) / (1.0 + jnp.exp(f))
        lf = log1p_neg(key)
        hi = lf.astype(BF16)
        lo = (lf - hi.astype(F32)).astype(BF16)
        t = tril[...]
        tb = t.astype(BF16)
        ones = jnp.ones((2 * BL, HK), BF16)
        cums = []
        for h in range(2):
            hc = slice(h * HK, (h + 1) * HK)
            te = t * extra[h : h + 1, b * BL : (b + 1) * BL]
            te_hi = te.astype(BF16)
            te_lo = (te - te_hi.astype(F32)).astype(BF16)
            lhs = jnp.concatenate([tb, tb, te_hi, te_lo], axis=1)
            rhs = jnp.concatenate([hi[:, hc], lo[:, hc], ones], axis=0)
            cums.append(dot(lhs, rhs))
        cum = jnp.concatenate(cums, axis=1)
        m = cum[BL // 2 - 1 : BL // 2, :]
        last = cum[BL - 1 : BL, :]
        rel = cum - m
        ebuf[r, :] = jnp.exp(rel)
        kd = key * jnp.exp(-rel)
        kbuf[r, :] = kd.astype(BF16)
        kst = (kd * jnp.exp(last - m)).astype(BF16)
        lpre = lrun[...]
        vecs[b, 0:1, :] = lpre
        vecs[b, 1:2, :] = m
        lrun[...] = lpre + last
        a = jnp.exp(last)
        v = vbuf[r, :]
        for h in range(2):
            hc = slice(h * HK, (h + 1) * HK)
            contrib = dot(v[:, hc], kst[:, hc], TN)
            s = run[h]
            sloc[b, h] = s
            run[h] = s * a[:, hc] + contrib

    def proj_p(i):
        r = pl.ds(i * CH, CH)
        pbuf[pl.ds(BL + i * CH, CH), :] = dot(nbuf[r, :], wp[...]).astype(BF16)

    def proj_qg(d):
        r = rows(d, OUT)
        o = dot(nbuf[r, :], wqg[...])
        q = o[:, :C]
        qbuf[r, :] = (q * half_tanh_sigmoid(q) * ebuf[r, :]).astype(BF16)
        g = o[:, C:]
        gbuf[r, :] = g * half_tanh_sigmoid(g) * rgain[...]

    def score_block(b):
        r = rows(b, BL)
        causal = tril[...] > 0.5
        for h in range(2):
            hc = slice(h * HK, (h + 1) * HK)
            s = dot(qbuf[r, hc], kbuf[r, hc], NT)
            s = jnp.where(causal, s, 0.0).astype(BF16)
            winbuf[r, hc] = dot(s, vbuf[r, hc])

    def pool_block(b):
        ext = pbuf[pl.ds(pl.multiple_of(b * BL, BL), 2 * BL), :]
        sums = dot(band[...], ext)
        t = sp * ROWS + b * BL + lax.broadcasted_iota(jnp.int32, (BL, 1), 0)
        cnt = jnp.minimum(t + 1, w).astype(F32)
        pooled = (sums / cnt - ext[BL:, :].astype(F32)).astype(BF16)
        return (dot(pooled, mix[0]) * pscale[...]).astype(BF16)

    def out_block(b):
        r = pl.ds(pl.multiple_of(b * BL, BL), BL)
        lpre = vecs[b, 0:1, :]
        m = vecs[b, 1:2, :]
        em = jnp.exp(m)
        elm = jnp.exp(lpre + m)
        parts = []
        for h in range(2):
            hc = slice(h * HK, (h + 1) * HK)
            st = (sloc[b, h] * em[:, hc] + carr[h] * elm[:, hc]).astype(BF16)
            o = winbuf[r, hc] + dot(qbuf[r, hc], st, NT)
            ms = jnp.sum(o * o, axis=-1, keepdims=True) * (1.0 / HK)
            parts.append(o * lax.rsqrt(ms + EPS) * gbuf[r, hc])
        return jnp.concatenate(parts, axis=1).astype(BF16)

    def chain(ea, eS, la, lS):
        return ea * la, la * eS + lS

    def put_state(ref, a, S):
        hi = a.astype(BF16)
        lo = (a - hi.astype(F32)).astype(BF16)
        ref[0:HK, :] = S.astype(BF16)
        ref[HK : HK + 8, :] = jnp.broadcast_to(hi, (8, HK))
        ref[HK + 8 : HK + 16, :] = jnp.broadcast_to(lo, (8, HK))

    def scan_states(ref, me):
        ta = jnp.ones((1, HK), F32)
        tS = jnp.zeros((HK, HK), F32)
        pa_, pS_ = ta, tS
        for j in range(4):
            full = ref[j].astype(F32)
            ta, tS = chain(ta, tS, full[HK : HK + 1, :] + full[HK + 8 : HK + 9, :], full[0:HK, :])
            pa_ = jnp.where(me > j, ta, pa_)
            pS_ = jnp.where(me > j, tS, pS_)
        return ta, tS, pa_, pS_

    w1, w2, w3 = {}, {}, {}

    def w1_send(k):
        for a, at in enumerate((pa, pb)):
            dst = wout.at[c, pl.ds(pl.multiple_of(x * 256 + at, 32), 32)]
            w1[k, a] = remote(wst.at[c, a], dst, w1s.at[k - 1, a], w1r.at[k - 1, a], xpeer(k))

    def w2_send(k, a):
        w1[k, a].wait_recv()
        j = lax.rem(x + 4 - k, 4)
        sl = wout.at[c, pl.ds(pl.multiple_of(j * 256 + (pb if a else pa), 32), 32)]
        for q in (2, 1, 3):
            to = (zpeer if a else ypeer)(q)
            w2[k, a, q] = remote(sl, sl, w2s.at[a, k - 1, q - 1], w2r.at[a, k - 1, q - 1], to)

    def w3_send(k, a):
        for q in (1, 2, 3):
            w2[k, a, q].wait_recv()
        j = lax.rem(x + 4 - k, 4)
        sl = wout.at[c, pl.ds(pl.multiple_of(j * 256 + a * 128, 128), 128)]
        w3[k, a] = remote(sl, sl, w3s.at[a, k - 1], w3r.at[a, k - 1], sib)

    l_gain.wait()
    l_x[0].wait()
    norm(0)
    run[...] = jnp.zeros_like(run)
    lrun[...] = jnp.zeros_like(lrun)
    pbuf[pl.ds(0, BL - 16), :] = jnp.zeros((BL - 16, C), BF16)
    l_wf.wait()
    l_wv.wait()
    l_lb.wait()
    l_extra.wait()
    for i in range(NCH):
        if i + 1 < NCH:
            l_x[i + 1].wait()
        proj_fv(i)
        if i + 1 < NCH:
            norm(i + 1)
        if i > 0:
            state_block(2 * i - 2)
            state_block(2 * i - 1)
        if i == 0:
            for cp in l_pc:
                cp.wait()
            pl.semaphore_wait(bar, 12)
            w1_send(1)
            w1_send(3)
            w1_send(2)
        if i == 4:
            w2_send(1, 0)
    state_block(NB - 2)
    state_block(NB - 1)
    w2_send(1, 1)

    for h in range(2):
        totsend[h, 0:HK, :] = run[h]
        al = jnp.exp(lrun[:, h * HK : (h + 1) * HK])
        totsend[h, HK : HK + 8, :] = jnp.broadcast_to(al, (8, HK))
    e_cp = remote(totsend, totrecv, es, er, sib)

    l_p.wait()
    for i in (5, 0, 1):
        proj_p(i)
    h_cp = remote(pbuf.at[pl.ds(BL + ROWS - 16, 16)], pbuf.at[pl.ds(BL - 16, 16)], hs, hr, nxt)
    e_cp.wait()
    oS, oa = totsend[c, 0:HK, :], totsend[c, HK : HK + 1, :]
    sS, sa = totrecv[c, 0:HK, :], totrecv[c, HK : HK + 1, :]
    first = c == 0
    ea, eS = jnp.where(first, oa, sa), jnp.where(first, oS, sS)
    la, lS = jnp.where(first, sa, oa), jnp.where(first, sS, oS)
    put_state(ybuf.at[y], *chain(ea, eS, la, lS))
    y_cp = [
        remote(ybuf.at[y], ybuf.at[y], ys.at[k - 1], yr_.at[k - 1], ypeer(k)) for k in (2, 1, 3)
    ]
    for i in (2, 3, 4):
        proj_p(i)
    l_ps.wait()
    l_mix.wait()
    h_cp.wait()

    @pl.when(sp == 0)
    def _():
        pbuf[pl.ds(BL - 16, 16), :] = jnp.zeros((16, C), BF16)

    ap = []
    for k in (2, 1, 3, 0):
        d = lax.rem(x + k, 4)
        for s in range(3):
            blk = pool_block(d * 3 + s)
            if k == 0:
                ypseen[x, pl.ds(s * BL, BL), :] = blk
            else:
                ypbuf[k - 1, pl.ds(s * BL, BL), :] = blk
        if k:
            ap.append(remote(ypbuf.at[k - 1], ypseen.at[x], aps.at[k - 1], apr.at[k - 1], xpeer(k)))

    def do_qg(k):
        d = lax.rem(x + k, 4)
        proj_qg(d)
        for s in range(3):
            score_block(d * 3 + s)

    ar = []

    def do_out(k):
        d = lax.rem(x + k, 4)
        for s in range(3):
            blk = out_block(d * 3 + s)
            if k == 0:
                yrseen[x, pl.ds(s * BL, BL), :] = blk
            else:
                yrbuf[k - 1, pl.ds(s * BL, BL), :] = blk
        if k:
            ar.append(remote(yrbuf.at[k - 1], yrseen.at[x], ars.at[k - 1], arr.at[k - 1], xpeer(k)))

    l_q.wait()
    l_g.wait()
    l_rg.wait()
    for cp in y_cp:
        cp.wait()
    ta, tS, ya, yS = scan_states(ybuf, y)
    put_state(zbuf.at[z], ta, tS)
    pst[0:HK, :] = yS
    pst[HK : HK + 8, :] = jnp.broadcast_to(ya, (8, HK))
    z_cp = [
        remote(zbuf.at[z], zbuf.at[z], zs.at[k - 1], zr.at[k - 1], zpeer(k)) for k in (2, 1, 3)
    ]
    w2_send(3, 0)
    w2_send(2, 0)
    do_qg(2)
    for cp in z_cp:
        cp.wait()
    ta, tS, za, zS = scan_states(zbuf, z)
    l_init.wait()
    fa, fS = chain(za, zS, pst[HK : HK + 1, :], pst[0:HK, :])
    carr[c] = fa * jnp.transpose(init[c]) + fS
    p_cp = remote(carr.at[c], carr.at[c], ps_, pr_, sib)
    w2_send(3, 1)
    w2_send(2, 1)
    do_qg(1)
    p_cp.wait()
    for h in range(2):
        pcur = carr[h]
        later = totrecv[h, HK : HK + 1, :] * pcur + totrecv[h, 0:HK, :]
        carr[h] = jnp.where(c == 0, pcur, later)
    do_out(2)
    do_out(1)
    w3_send(1, 0)
    w3_send(1, 1)
    do_qg(3)
    do_out(3)
    do_qg(0)
    do_out(0)

    w3_send(3, 0)
    w3_send(2, 0)
    w3_send(3, 1)
    w3_send(2, 1)
    for cp in w3.values():
        cp.wait()
    for cp in w1.values():
        cp.wait_send()
    for cp in w2.values():
        cp.wait_send()
    l_op.wait()
    l_or.wait()
    for cp in ap:
        cp.wait()
    yp = jnp.concatenate([ypseen[j] for j in range(4)], axis=1)
    for n in range(4):
        nc = pl.ds(n * 512, 512)
        acc[:, nc] = dot(yp, wout[0, :, nc])
    for cp in ar:
        cp.wait()
    yr = jnp.concatenate([yrseen[j] for j in range(4)], axis=1)
    for n in range(4):
        nc = pl.ds(n * 512, 512)
        out_ref[:, nc] = (acc[:, nc] + dot(yr, wout[1, :, nc])).astype(BF16)


def scratch():
    V = pltpu.VMEM
    S = pltpu.SemaphoreType.DMA
    return [
        V((ROWS, D), BF16), V((ROWS, D), BF16), V((D, 2 * C), BF16), V((D, 2 * C), BF16), V((D, C), BF16),
        V((2, 2, 32, D), BF16),
        V((2, 4 * C, D), BF16), V((1, D), F32), V((1, C), F32), V((1, C), F32), V((1, C), F32),
        V((2, ROWS), F32), V((1, C, C), BF16), V((2, HK, HK), F32),
        V((ROWS, C), F32), V((ROWS, C), BF16), V((ROWS, C), F32), V((ROWS, C), BF16),
        V((ROWS, C), BF16), V((ROWS, C), F32), V((ROWS, C), F32), V((BL + ROWS, C), BF16),
        V((NB, 2, HK, HK), F32), V((2, HK, HK), F32), V((1, C), F32), V((NB, 2, C), F32),
        V((2, HK + 8, HK), F32), V((2, HK + 8, HK), F32), V((4, HK + 16, HK), BF16), V((4, HK + 16, HK), BF16),
        V((HK + 8, HK), F32), V((2, HK, HK), F32), V((BL, BL), F32), V((BL, 2 * BL), BF16),
        V((3, OUT, C), BF16), V((4, OUT, C), BF16), V((3, OUT, C), BF16), V((4, OUT, C), BF16),
        V((OUT, D), F32),
        S((24,)), S((3, 2)), S((3, 2)), S((2, 3, 3)), S((2, 3, 3)), S((2, 3)), S((2, 3)),
        S(()), S(()), S((3,)), S((3,)), S((3,)), S((3,)), S(()), S(()), S(()), S(()),
        S((3,)), S((3,)), S((3,)), S((3,)),
    ]


def per_device(
    inputs, norm_gain, pool_weight, query_weight, forget_weight, value_weight, outgate_weight,
    pool_mix, pool_scale, lower_bound, extra_decay, recur_gain, init_state, out_pool, out_recur,
):
    anyspec = pl.BlockSpec(memory_space=pl.ANY)
    return pl.pallas_call(
        kernel,
        out_shape=jax.ShapeDtypeStruct((OUT, D), BF16),
        in_specs=[anyspec] * 15,
        out_specs=pl.BlockSpec(memory_space=pltpu.VMEM),
        scratch_shapes=scratch(),
        compiler_params=pltpu.CompilerParams(
            collective_id=0, has_side_effects=True, vmem_limit_bytes=63 * 1024 * 1024
        ),
    )(
        inputs, norm_gain.reshape(1, D), pool_weight, query_weight, forget_weight, value_weight,
        outgate_weight, pool_mix, pool_scale.reshape(1, C), lower_bound.reshape(1, C),
        extra_decay.T, recur_gain.reshape(1, C), init_state, out_pool, out_recur,
    )


def solution(mesh):
    placed = (
        P("sp", None), P(), P(None, "tp"), P(None, "tp"), P(None, "tp"), P(None, "tp"), P(None, "tp"),
        P("tp", None, None), P("tp"), P("tp"), P("sp", "tp"), P("tp"), P("tp", None, None),
        P("tp", None), P("tp", None),
    )
    return jax.shard_map(
        per_device, mesh=mesh, in_specs=placed, out_specs=P(("sp", "tp"), None), check_vma=False
    )
```

```python
import jax
import jax.numpy as jnp
from jax import lax
from jax.experimental import pallas as pl
from jax.experimental.pallas import tpu as pltpu
from jax.sharding import PartitionSpec as P

MESH = pl.DeviceIdType.MESH
F32 = jnp.float32
BF16 = jnp.bfloat16
EPS = 1e-5

ROWS = 1536
OUT = 384
BL = 128
NB = ROWS // BL
C = 256
HK = 128
D = 2048
PF = HK + 16

NT = (((1,), (1,)), ((), ()))
TN = (((0,), (0,)), ((), ()))
NN = (((1,), (0,)), ((), ()))

LOG2E = 1.4426950408889634
POLY = (-LOG2E, -0.7213472908955184, -0.48097089760573397, -0.3571200043786398, -0.3431147843908393)


def dot(a, b, dims=NN):
    return lax.dot_general(a, b, dims, preferred_element_type=F32)


def silu(v):
    half = 0.5 * v
    return half + half * jnp.tanh(half)


def twice(a):
    return jnp.concatenate([a, a], axis=1)


def diag2(a, b):
    zero = jnp.zeros((HK, HK), BF16)
    top = jnp.concatenate([a, zero], axis=1)
    return jnp.concatenate([top, jnp.concatenate([zero, b], axis=1)], axis=0)


def kernel(
    x_hbm, gain_hbm, wp_hbm, wq_hbm, wf_hbm, wv_hbm, wg_hbm, mix_hbm, pscale_hbm, lb_hbm,
    extra_hbm, rgain_hbm, init_hbm, op_hbm, or_hbm,
    out_ref,
    xbuf, nbuf, wf, wv, wq, wg, wp, wst, wout, gain, pscale, lb, rgain, extra, mix, init,
    rsbuf, ecum, fbuf, vbuf, ebuf, kdiag, vdiag, qbuf, winbuf, gbuf, pbuf, sloc, run, lrun, vecs,
    totsend, totrecv, ybuf, zbuf, pst, carr, trilb, band,
    ypbuf, ypseen, yrbuf, yrseen, acc, obuf,
    lsem, w1s, w1r, w1fs, w1fr, w2s, w2r, w2fs, w2fr, w3s, w3r,
    es, er, ys, yr_, zs, zr, cs, cr, hs, hr, aps, apr, ars, arr, osem,
):
    x = lax.axis_index("tp")
    sp = lax.axis_index("sp")
    c = lax.rem(sp, 2)
    chip = lax.div(sp, 2)
    y = lax.rem(chip, 4)
    z = lax.div(chip, 4)

    def dev(spi, tpi):
        return {"sp": spi, "tp": tpi}

    def xpeer(k):
        return dev(sp, lax.rem(x + k, 4))

    def ypeer(k):
        return dev(z * 8 + lax.rem(y + k, 4) * 2 + c, x)

    def zpeer(k):
        return dev(lax.rem(z + k, 4) * 8 + y * 2 + c, x)

    sib = dev(sp + 1 - 2 * c, x)
    nxt = dev(lax.rem(sp + 1, 32), x)
    prv = dev(lax.rem(sp + 31, 32), x)

    count = [0]

    def load(src, dst):
        i = count[0]
        count[0] += 1
        cp = pltpu.make_async_copy(src, dst, lsem.at[i])
        cp.start()
        return cp

    def remote(src, dst, ssem, rsem, to, start=True):
        cp = pltpu.make_async_remote_copy(
            src_ref=src, dst_ref=dst, send_sem=ssem, recv_sem=rsem, device_id=to, device_id_type=MESH
        )
        if start:
            cp.start()
        return cp

    def rows(i, n):
        return pl.ds(pl.multiple_of(i * n, n), n)

    pa = pl.multiple_of(y * 32, 32)
    pb = pl.multiple_of(128 + z * 32, 32)
    l_extra = load(extra_hbm, extra)
    l_gain = load(gain_hbm, gain)
    l_x = [load(x_hbm.at[pl.ds(0, OUT)], xbuf.at[pl.ds(0, OUT)])]
    l_wf = load(wf_hbm, wf)
    l_wv = load(wv_hbm, wv)
    l_lb = load(lb_hbm, lb)
    l_x.append(load(x_hbm.at[pl.ds(OUT, OUT)], xbuf.at[pl.ds(OUT, OUT)]))
    l_pc = [load(op_hbm.at[pl.ds(pa, 32)], wst.at[0, 0]), load(op_hbm.at[pl.ds(pb, 32)], wst.at[0, 1])]
    l_pc += [load(or_hbm.at[pl.ds(pa, 32)], wst.at[1, 0]), load(or_hbm.at[pl.ds(pb, 32)], wst.at[1, 1])]
    bar = pltpu.get_barrier_semaphore()
    for k in (1, 2, 3):
        for peer in (xpeer, ypeer, zpeer):
            pl.semaphore_signal(bar, inc=1, device_id=peer(k), device_id_type=MESH)
    for to in (sib, nxt, prv):
        pl.semaphore_signal(bar, inc=1, device_id=to, device_id_type=MESH)

    def extra_sums(b):
        parts = []
        for h in range(2):
            e = extra[h : h + 1, b * BL : (b + 1) * BL] * LOG2E
            hi = e.astype(BF16)
            lo = (e - hi.astype(F32)).astype(BF16)
            t = trilb[...]
            parts.append(jnp.concatenate([t * hi, t * lo], axis=1))
        o = dot(jnp.concatenate(parts, axis=0), jnp.ones((2 * BL, HK), BF16))
        r = pl.ds(b * BL, BL)
        ecum[r, 0:HK] = o[:BL]
        ecum[r, HK:] = o[BL:]

    def norm(j):
        g = gain[...].astype(BF16)
        sums = []
        for s in range(3):
            r = pl.ds(j * OUT + s * BL, BL)
            v = xbuf[r, :]
            nbuf[r, :] = v * g
            sq = v * v
            t = [sq[:, i * 256 : (i + 1) * 256] for i in range(8)]
            while len(t) > 1:
                t = [t[i] + t[i + 1] for i in range(0, len(t), 2)]
            sums.append(t[0])
        ss = dot(jnp.concatenate(sums, axis=0), jnp.ones((256, HK), BF16))
        rsbuf[pl.ds(j * OUT, OUT), :] = lax.rsqrt(ss * (1.0 / D) + EPS)

    def proj_fv(j):
        r = pl.ds(j * OUT, OUT)
        n = nbuf[r, :]
        rs = twice(rsbuf[r, :])
        fbuf[r, :] = dot(n, wf[...]) * (0.5 * rs)
        vbuf[r, :] = (dot(n, wv[...]) * rs).astype(BF16)

    def state_block(b):
        r = pl.ds(b * BL, BL)
        half = 0.5 * (1.0 - lb[...])
        key = half - half * jnp.tanh(fbuf[r, :])
        lf = POLY[4] * key + POLY[3]
        for n in (2, 1, 0):
            lf = lf * key + POLY[n]
        lf = lf * key
        hi = lf.astype(BF16)
        lo = (lf - hi.astype(F32)).astype(BF16)
        t = trilb[...]
        cum = dot(twice(t), jnp.concatenate([hi, lo], axis=0)) + ecum[r, :]
        m = cum[BL // 2 - 1 : BL // 2, :]
        last = cum[BL - 1 : BL, :]
        rel = cum - m
        ebuf[r, :] = jnp.exp2(rel)
        kd = (key * jnp.exp2(-rel)).astype(BF16)
        v = vbuf[r, :]
        for h in range(2):
            hc = slice(h * HK, (h + 1) * HK)
            kdiag[b, hc, hc] = kd[:, hc]
            vdiag[b, hc, hc] = v[:, hc]
        lpre = lrun[...]
        vecs[b, 0:1, :] = lpre
        vecs[b, 1:2, :] = m
        lrun[...] = lpre + last
        a = jnp.exp2(last)
        e2 = jnp.exp2(last - m)
        contrib = dot(v, kd, TN)
        for h in range(2):
            hc = slice(h * HK, (h + 1) * HK)
            s = run[h]
            sloc[b, h] = s
            run[h] = s * a[:, hc] + contrib[hc, hc] * e2[:, hc]

    def proj_p(i):
        r = pl.ds(i * OUT, OUT)
        o = dot(nbuf[r, :], wp[...]) * twice(rsbuf[r, :])
        pbuf[pl.ds(BL + i * OUT, OUT), :] = o.astype(BF16)

    def proj_qg(d):
        r = rows(d, OUT)
        n = nbuf[r, :]
        rs = twice(rsbuf[r, :])
        qbuf[r, :] = (silu(dot(n, wq[...]) * rs) * ebuf[r, :]).astype(BF16)
        gbuf[r, :] = silu(dot(n, wg[...]) * rs) * rgain[...]

    def score_block(b):
        r = rows(b, BL)
        s = dot(qbuf[r, :], kdiag[b], NT)
        s = jnp.where(twice(trilb[...]) > 0, s, 0.0).astype(BF16)
        winbuf[r, :] = dot(s, vdiag[b])

    def pool_rows(d):
        parts = []
        for s in range(3):
            b = d * 3 + s
            ext = pbuf[pl.ds(pl.multiple_of(b * BL, BL), 2 * BL), :]
            sums = dot(band[...], ext)
            t = sp * ROWS + b * BL + lax.broadcasted_iota(jnp.int32, (BL, 1), 0)
            cnt = jnp.minimum(t + 1, w).astype(F32)
            parts.append((sums * (1.0 / cnt) - ext[BL:, :].astype(F32)).astype(BF16))
        return (dot(jnp.concatenate(parts, axis=0), mix[0]) * pscale[...]).astype(BF16)

    def out_block(b):
        r = rows(b, BL)
        lpre = vecs[b, 0:1, :]
        m = vecs[b, 1:2, :]
        em = jnp.exp2(m)
        elm = jnp.exp2(lpre + m)
        st = [
            (sloc[b, h] * em[:, h * HK : (h + 1) * HK] + carr[h] * elm[:, h * HK : (h + 1) * HK]).astype(BF16)
            for h in range(2)
        ]
        o = winbuf[r, :] + dot(qbuf[r, :], diag2(st[0], st[1]), NT)
        g = gbuf[r, :]
        parts = []
        for h in range(2):
            hc = slice(h * HK, (h + 1) * HK)
            oh = o[:, hc]
            ms = jnp.sum(oh * oh, axis=-1, keepdims=True) * (1.0 / HK)
            parts.append(oh * lax.rsqrt(ms + EPS) * g[:, hc])
        return jnp.concatenate(parts, axis=1).astype(BF16)

    def chain(ea, eS, la, lS):
        return ea * la, la * eS + lS

    def put_state(ref, a, S):
        hi = a.astype(BF16)
        lo = (a - hi.astype(F32)).astype(BF16)
        ref[0:HK, :] = S.astype(BF16)
        ref[HK : HK + 8, :] = jnp.broadcast_to(hi, (8, HK))
        ref[HK + 8 : HK + 16, :] = jnp.broadcast_to(lo, (8, HK))

    def scan_states(ref, me):
        ta = jnp.ones((1, HK), F32)
        tS = jnp.zeros((HK, HK), F32)
        ea, eS = ta, tS
        for j in range(4):
            full = ref[j].astype(F32)
            ta, tS = chain(ta, tS, full[HK : HK + 1, :] + full[HK + 8 : HK + 9, :], full[0:HK, :])
            ea = jnp.where(me > j, ta, ea)
            eS = jnp.where(me > j, tS, eS)
        return ta, tS, ea, eS

    w1, w1f, w2, w2f, w3 = {}, {}, {}, {}, {}

    def shard_of(k):
        return lax.rem(x + 4 - k, 4)

    def piece(k, a, at, half=None):
        start = shard_of(k) * 256 + a * 128 + at * 32
        if half is None:
            return wout.at[c, pl.ds(pl.multiple_of(start, 32), 32)]
        return wout.at[c, pl.ds(pl.multiple_of(start + half * 16, 16), 16)]

    def mine(a):
        return z if a else y

    def w1_send():
        for a in (1, 0):
            for k in (1, 3):
                w1[k, a] = remote(
                    wst.at[c, a], piece(0, a, mine(a)), w1s.at[k // 2, a], w1r.at[k // 2, a], xpeer(k)
                )

    def w2_first(k, a):
        for q in (1, 3):
            sl = piece(k, a, mine(a))
            to = (zpeer if a else ypeer)(q)
            w2[k, a, q] = remote(sl, sl, w2s.at[a, k - 1, q // 2], w2r.at[a, k - 1, q // 2], to)

    def w1_poll(k, a):
        w1[k, a].wait_recv()
        h = k // 2
        sl = piece(k, a, mine(a), h)
        w1f[h, a] = remote(sl, sl, w1fs.at[h, a], w1fr.at[h, a], xpeer(k))
        w2_first(k, a)

    def w1_poll2(a):
        for h in range(2):
            w1f[h, a].wait_recv()
        w2_first(2, a)

    def w2_poll(k, a):
        for h, q in enumerate((1, 3)):
            w2[k, a, q].wait_recv()
            sl = piece(k, a, lax.rem(mine(a) + 4 - q, 4), h)
            to = (zpeer if a else ypeer)(q)
            w2f[k, a, h] = remote(sl, sl, w2fs.at[a, k - 1, h], w2fr.at[a, k - 1, h], to)
        for q in (0, 1, 3):
            w3_send(k, a, q)

    def w3_send(k, a, q):
        sl = piece(k, a, lax.rem(mine(a) + q, 4))
        w3[k, a, q] = remote(sl, sl, w3s.at[a, k - 1, q], w3r.at[a, k - 1, q], sib)

    def w3_poll(k, a):
        for h in range(2):
            w2f[k, a, h].wait_recv()
        w3_send(k, a, 2)

    r_i = lax.broadcasted_iota(jnp.int32, (BL, BL), 0)
    c_i = lax.broadcasted_iota(jnp.int32, (BL, BL), 1)
    trilb[...] = jnp.where(c_i <= r_i, 1.0, 0.0).astype(BF16)
    w = lax.shift_left(jnp.int32(2), x)
    r_w = lax.broadcasted_iota(jnp.int32, (BL, 2 * BL), 0)
    c_w = lax.broadcasted_iota(jnp.int32, (BL, 2 * BL), 1)
    diff = r_w + BL - c_w
    band[...] = jnp.where((diff >= 0) & (diff < w), 1.0, 0.0).astype(BF16)
    run[...] = jnp.zeros_like(run)
    lrun[...] = jnp.zeros_like(lrun)
    pbuf[pl.ds(0, BL - 16), :] = jnp.zeros((BL - 16, C), BF16)
    for b in range(NB):
        for h in range(2):
            hc, oc = slice(h * HK, (h + 1) * HK), slice((1 - h) * HK, (2 - h) * HK)
            kdiag[b, hc, oc] = jnp.zeros((HK, HK), BF16)
            vdiag[b, hc, oc] = jnp.zeros((HK, HK), BF16)
    l_extra.wait()
    for b in range(NB):
        extra_sums(b)

    l_gain.wait()
    l_x[0].wait()
    norm(0)
    l_wf.wait()
    l_wv.wait()
    l_lb.wait()
    for i in range(2, 4):
        l_x.append(load(x_hbm.at[pl.ds(i * OUT, OUT)], xbuf.at[pl.ds(i * OUT, OUT)]))
    l_p = load(wp_hbm, wp)
    l_q = load(wq_hbm, wq)
    l_g = load(wg_hbm, wg)
    l_init = load(init_hbm, init)
    l_rg = load(rgain_hbm, rgain)
    l_ps = load(pscale_hbm, pscale)
    l_mix = load(mix_hbm, mix)
    l_op = load(op_hbm, wout.at[0, rows(x, 256)])
    l_or = load(or_hbm, wout.at[1, rows(x, 256)])
    for i in range(4):
        if i < 3:
            l_x[i + 1].wait()
        proj_fv(i)
        if i < 3:
            norm(i + 1)
        if i > 0:
            for s in range(3):
                state_block(3 * i - 3 + s)
        if i == 0:
            for cp in l_pc:
                cp.wait()
            pl.semaphore_wait(bar, 12)
            w1_send()
    for s in range(3):
        state_block(9 + s)

    for h in range(2):
        totsend[h, 0:HK, :] = run[h]
        al = jnp.exp2(lrun[:, h * HK : (h + 1) * HK])
        totsend[h, HK : HK + 8, :] = jnp.broadcast_to(al, (8, HK))
    e_cp = remote(totsend, totrecv, es, er, sib)

    w1_poll(1, 1)
    w1_poll(3, 1)
    l_p.wait()
    proj_p(3)
    proj_p(0)
    h_cp = remote(pbuf.at[pl.ds(BL + ROWS - 16, 16)], pbuf.at[pl.ds(BL - 16, 16)], hs, hr, nxt)
    e_cp.wait()
    oS, oa = totsend[c, 0:HK, :], totsend[c, HK : HK + 1, :]
    sS, sa = totrecv[c, 0:HK, :], totrecv[c, HK : HK + 1, :]
    first = c == 0
    ea, eS = jnp.where(first, oa, sa), jnp.where(first, oS, sS)
    la, lS = jnp.where(first, sa, oa), jnp.where(first, sS, oS)
    put_state(ybuf.at[y], *chain(ea, eS, la, lS))
    y_cp = [
        remote(ybuf.at[y], ybuf.at[y], ys.at[k - 1], yr_.at[k - 1], ypeer(k)) for k in (2, 1, 3)
    ]
    w1_poll(1, 0)
    w1_poll(3, 0)
    proj_p(1)
    proj_p(2)
    l_ps.wait()
    l_mix.wait()
    h_cp.wait()

    @pl.when(sp == 0)
    def _():
        pbuf[pl.ds(BL - 16, 16), :] = jnp.zeros((16, C), BF16)

    ap = []
    for k in (2, 1, 3, 0):
        blk = pool_rows(lax.rem(x + k, 4))
        if k:
            ypbuf[k - 1] = blk
            ap.append(remote(ypbuf.at[k - 1], ypseen.at[x], aps.at[k - 1], apr.at[k - 1], xpeer(k)))
        else:
            ypseen[x] = blk

    def do_proj(k):
        proj_qg(lax.rem(x + k, 4))

    def do_scores(k):
        for s in range(3):
            score_block(lax.rem(x + k, 4) * 3 + s)

    def do_qg(k):
        do_proj(k)
        do_scores(k)

    ar = {}

    def do_out(k):
        d = lax.rem(x + k, 4)
        for s in range(3):
            blk = out_block(d * 3 + s)
            if k == 0:
                yrseen[x, pl.ds(s * BL, BL), :] = blk
            else:
                yrbuf[k - 1, pl.ds(s * BL, BL), :] = blk
        if k:
            ar[k] = remote(yrbuf.at[k - 1], yrseen.at[x], ars.at[k - 1], arr.at[k - 1], xpeer(k))

    l_q.wait()
    l_g.wait()
    l_rg.wait()
    do_proj(1)
    for cp in y_cp:
        cp.wait()
    ta, tS, ya, yS = scan_states(ybuf, y)
    put_state(zbuf.at[z], ta, tS)
    pst[0:HK, :] = yS
    pst[HK : HK + 8, :] = jnp.broadcast_to(ya, (8, HK))
    z_cp = [
        remote(zbuf.at[z], zbuf.at[z], zs.at[k - 1], zr.at[k - 1], zpeer(k)) for k in (2, 1, 3)
    ]
    do_scores(1)
    w1_poll2(1)
    w2_poll(1, 1)
    do_qg(3)
    w2_poll(3, 1)
    w1_poll2(0)
    do_qg(2)
    w2_poll(1, 0)
    for cp in z_cp:
        cp.wait()
    ta, tS, za, zS = scan_states(zbuf, z)
    l_init.wait()
    fa, fS = chain(za, zS, pst[HK : HK + 1, :], pst[0:HK, :])
    carr[c] = fa * jnp.transpose(init[c]) + fS
    c_cp = remote(carr.at[c], carr.at[c], cs, cr, sib)
    do_qg(0)
    w2_poll(3, 0)
    w2_poll(2, 1)
    c_cp.wait()
    for h in range(2):
        cur = carr[h]
        later = totrecv[h, HK : HK + 1, :] * cur + totrecv[h, 0:HK, :]
        carr[h] = jnp.where(c == 0, cur, later)
    do_out(1)
    do_out(3)
    do_out(2)
    w3_poll(1, 1)
    w3_poll(3, 1)
    do_out(0)
    w3_poll(1, 0)
    w3_poll(3, 0)
    w2_poll(2, 0)
    l_op.wait()
    l_or.wait()
    for k in (1, 3):
        for a in range(2):
            for q in range(4):
                w3[k, a, q].wait()
    for cp in ap:
        cp.wait()

    def out_dot(parts, nc):
        left = [(yrseen if mat else ypseen)[shard_of(k)] for mat, k in parts]
        right = [wout[mat, rows(shard_of(k), 256), nc] for mat, k in parts]
        return dot(jnp.concatenate(left, axis=1), jnp.concatenate(right, axis=0))

    for n in range(4):
        nc = pl.ds(n * 512, 512)
        acc[:, nc] = out_dot(((0, 0), (0, 1), (0, 3), (1, 0)), nc)
    w3_poll(2, 1)
    w3_poll(2, 0)
    ar[1].wait()
    ar[3].wait()
    for a in range(2):
        for q in range(4):
            w3[2, a, q].wait()
    for n in range(4):
        nc = pl.ds(n * 512, 512)
        acc[:, nc] += out_dot(((0, 2), (1, 1), (1, 3)), nc)
    ar[2].wait()
    outs = []
    for n in range(4):
        nc = pl.ds(n * 512, 512)
        obuf[n] = (acc[:, nc] + out_dot(((1, 2),), nc)).astype(BF16)
        cp = pltpu.make_async_copy(obuf.at[n], out_ref.at[:, nc], osem.at[n])
        cp.start()
        outs.append(cp)
    for group in (w1, w1f, w2, w2f):
        for cp in group.values():
            cp.wait_send()
    for cp in outs:
        cp.wait()


def scratch():
    V = pltpu.VMEM
    S = pltpu.SemaphoreType.DMA
    return [
        V((ROWS, D), BF16), V((ROWS, D), BF16), V((D, C), BF16), V((D, C), BF16), V((D, C), BF16),
        V((D, C), BF16), V((D, C), BF16),         V((2, 2, 32, D), BF16), V((2, 4 * C, D), BF16),
        V((1, D), F32), V((1, C), F32), V((1, C), F32), V((1, C), F32),
        V((2, ROWS), F32), V((1, C, C), BF16), V((2, HK, HK), F32),
        V((ROWS, HK), F32), V((ROWS, C), F32), V((ROWS, C), F32), V((ROWS, C), BF16), V((ROWS, C), F32),
        V((NB, C, C), BF16), V((NB, C, C), BF16), V((ROWS, C), BF16), V((ROWS, C), F32), V((ROWS, C), F32),
        V((BL + ROWS, C), BF16), V((NB, 2, HK, HK), F32), V((2, HK, HK), F32), V((1, C), F32), V((NB, 2, C), F32),
        V((2, HK + 8, HK), F32), V((2, HK + 8, HK), F32), V((4, PF, HK), BF16), V((4, PF, HK), BF16), V((HK + 8, HK), F32), V((2, HK, HK), F32),
        V((BL, BL), BF16), V((BL, 2 * BL), BF16),
        V((3, OUT, C), BF16), V((4, OUT, C), BF16), V((3, OUT, C), BF16), V((4, OUT, C), BF16),
        V((OUT, D), F32), V((4, OUT, 512), BF16),
        S((24,)), S((2, 2)), S((2, 2)), S((2, 2)), S((2, 2)), S((2, 3, 2)), S((2, 3, 2)), S((2, 3, 2)), S((2, 3, 2)),
        S((2, 3, 4)), S((2, 3, 4)),
        S(()), S(()), S((3,)), S((3,)), S((3,)), S((3,)), S(()), S(()), S(()), S(()), S((3,)), S((3,)), S((3,)), S((3,)),
        S((4,)),
    ]


def per_device(
    inputs, norm_gain, pool_weight, query_weight, forget_weight, value_weight, outgate_weight,
    pool_mix, pool_scale, lower_bound, extra_decay, recur_gain, init_state, out_pool, out_recur,
):
    anyspec = pl.BlockSpec(memory_space=pl.ANY)
    return pl.pallas_call(
        kernel,
        out_shape=jax.ShapeDtypeStruct((OUT, D), BF16),
        in_specs=[anyspec] * 15,
        out_specs=anyspec,
        scratch_shapes=scratch(),
        compiler_params=pltpu.CompilerParams(
            collective_id=0, has_side_effects=True, vmem_limit_bytes=63 * 1024 * 1024
        ),
    )(
        inputs, norm_gain.reshape(1, D), pool_weight, query_weight, forget_weight, value_weight,
        outgate_weight, pool_mix, pool_scale.reshape(1, C), lower_bound.reshape(1, C),
        extra_decay.T, recur_gain.reshape(1, C), init_state, out_pool, out_recur,
    )


def solution(mesh):
    placed = (
        P("sp", None), P(), P(None, "tp"), P(None, "tp"), P(None, "tp"), P(None, "tp"), P(None, "tp"),
        P("tp", None, None), P("tp"), P("tp"), P("sp", "tp"), P("tp"), P("tp", None, None),
        P("tp", None), P("tp", None),
    )
    return jax.shard_map(
        per_device, mesh=mesh, in_specs=placed, out_specs=P(("sp", "tp"), None), check_vma=False
    )
```

```python
import jax
import jax.numpy as jnp
from jax import lax
from jax.experimental import pallas as pl
from jax.experimental.pallas import tpu as pltpu
from jax.sharding import PartitionSpec as P

MESH = pl.DeviceIdType.MESH
F32 = jnp.float32
BF16 = jnp.bfloat16
EPS = 1e-5

ROWS = 1536
OUT = 384
BL = 128
NB = ROWS // BL
C = 256
HK = 128
D = 2048
PF = HK + 16

NT = (((1,), (1,)), ((), ()))
TN = (((0,), (0,)), ((), ()))
NN = (((1,), (0,)), ((), ()))

LOG2E = 1.4426950408889634
POLY = (-LOG2E, -0.7213472908955184, -0.48097089760573397, -0.3571200043786398, -0.3431147843908393)


def dot(a, b, dims=NN):
    return lax.dot_general(a, b, dims, preferred_element_type=F32)


def silu(v):
    half = 0.5 * v
    return half + half * jnp.tanh(half)


def twice(a):
    return jnp.concatenate([a, a], axis=1)


def diag2(a, b):
    zero = jnp.zeros((HK, HK), BF16)
    top = jnp.concatenate([a, zero], axis=1)
    return jnp.concatenate([top, jnp.concatenate([zero, b], axis=1)], axis=0)


def kernel(
    x_hbm, gain_hbm, wp_hbm, wq_hbm, wf_hbm, wv_hbm, wg_hbm, mix_hbm, pscale_hbm, lb_hbm,
    extra_hbm, rgain_hbm, init_hbm, op_hbm, or_hbm,
    out_ref,
    xbuf, nbuf, wf, wv, wq, wg, wp, wst, wout, gain, pscale, lb, rgain, extra, mix, init,
    rsbuf, ecum, fbuf, vbuf, ebuf, kdiag, vdiag, qbuf, winbuf, gbuf, pbuf, sloc, run, lrun, vecs,
    totsend, totrecv, ybuf, zbuf, pst, carr, trilb, band,
    ypbuf, ypseen, yrbuf, yrseen, acc, obuf,
    lsem, w1s, w1r, w1fs, w1fr, w2s, w2r, w2fs, w2fr, w3s, w3r,
    es, er, ys, yr_, zs, zr, cs, cr, hs, hr, aps, apr, ars, arr, osem,
):
    x = lax.axis_index("tp")
    sp = lax.axis_index("sp")
    c = lax.rem(sp, 2)
    chip = lax.div(sp, 2)
    y = lax.rem(chip, 4)
    z = lax.div(chip, 4)

    def dev(spi, tpi):
        return {"sp": spi, "tp": tpi}

    def xpeer(k):
        return dev(sp, lax.rem(x + k, 4))

    def ypeer(k):
        return dev(z * 8 + lax.rem(y + k, 4) * 2 + c, x)

    def zpeer(k):
        return dev(lax.rem(z + k, 4) * 8 + y * 2 + c, x)

    sib = dev(sp + 1 - 2 * c, x)
    nxt = dev(lax.rem(sp + 1, 32), x)
    prv = dev(lax.rem(sp + 31, 32), x)

    count = [0]

    def load(src, dst):
        i = count[0]
        count[0] += 1
        cp = pltpu.make_async_copy(src, dst, lsem.at[i])
        cp.start()
        return cp

    def remote(src, dst, ssem, rsem, to, start=True):
        cp = pltpu.make_async_remote_copy(
            src_ref=src, dst_ref=dst, send_sem=ssem, recv_sem=rsem, device_id=to, device_id_type=MESH
        )
        if start:
            cp.start()
        return cp

    def rows(i, n):
        return pl.ds(pl.multiple_of(i * n, n), n)

    pa = pl.multiple_of(y * 32, 32)
    pb = pl.multiple_of(128 + z * 32, 32)
    l_extra = load(extra_hbm, extra)
    l_gain = load(gain_hbm, gain)
    l_x = [load(x_hbm.at[pl.ds(0, OUT)], xbuf.at[pl.ds(0, OUT)])]
    l_wf = load(wf_hbm, wf)
    l_wv = load(wv_hbm, wv)
    l_lb = load(lb_hbm, lb)
    l_x.append(load(x_hbm.at[pl.ds(OUT, OUT)], xbuf.at[pl.ds(OUT, OUT)]))
    l_pc = [load(op_hbm.at[pl.ds(pa, 32)], wst.at[0, 0]), load(op_hbm.at[pl.ds(pb, 32)], wst.at[0, 1])]
    l_pc += [load(or_hbm.at[pl.ds(pa, 32)], wst.at[1, 0]), load(or_hbm.at[pl.ds(pb, 32)], wst.at[1, 1])]
    bar = pltpu.get_barrier_semaphore()
    for k in (1, 2, 3):
        for peer in (xpeer, ypeer, zpeer):
            pl.semaphore_signal(bar, inc=1, device_id=peer(k), device_id_type=MESH)
    pl.semaphore_signal(bar, inc=1, device_id=sib, device_id_type=MESH)

    @pl.when(sp < 31)
    def _():
        pl.semaphore_signal(bar, inc=1, device_id=nxt, device_id_type=MESH)

    @pl.when(sp > 0)
    def _():
        pl.semaphore_signal(bar, inc=1, device_id=prv, device_id_type=MESH)


    def extra_sums(b):
        parts = []
        for h in range(2):
            e = extra[h : h + 1, b * BL : (b + 1) * BL] * LOG2E
            hi = e.astype(BF16)
            lo = (e - hi.astype(F32)).astype(BF16)
            t = trilb[...]
            parts.append(jnp.concatenate([t * hi, t * lo], axis=1))
        o = dot(jnp.concatenate(parts, axis=0), jnp.ones((2 * BL, HK), BF16))
        r = pl.ds(b * BL, BL)
        ecum[r, 0:HK] = o[:BL]
        ecum[r, HK:] = o[BL:]

    def norm(j):
        g = gain[...].astype(BF16)
        sums = []
        for s in range(3):
            r = pl.ds(j * OUT + s * BL, BL)
            v = xbuf[r, :]
            nbuf[r, :] = v * g
            sq = v * v
            t = [sq[:, i * 256 : (i + 1) * 256] for i in range(8)]
            while len(t) > 1:
                t = [t[i] + t[i + 1] for i in range(0, len(t), 2)]
            sums.append(t[0])
        ss = dot(jnp.concatenate(sums, axis=0), jnp.ones((256, HK), BF16))
        rsbuf[pl.ds(j * OUT, OUT), :] = lax.rsqrt(ss * (1.0 / D) + EPS)

    def proj_fv(j):
        r = pl.ds(j * OUT, OUT)
        n = nbuf[r, :]
        rs = twice(rsbuf[r, :])
        fbuf[r, :] = dot(n, wf[...]) * (0.5 * rs)
        vbuf[r, :] = (dot(n, wv[...]) * rs).astype(BF16)

    def state_block(b):
        r = pl.ds(b * BL, BL)
        half = 0.5 * (1.0 - lb[...])
        key = half - half * jnp.tanh(fbuf[r, :])
        lf = POLY[4] * key + POLY[3]
        for n in (2, 1, 0):
            lf = lf * key + POLY[n]
        lf = lf * key
        hi = lf.astype(BF16)
        lo = (lf - hi.astype(F32)).astype(BF16)
        t = trilb[...]
        cum = dot(twice(t), jnp.concatenate([hi, lo], axis=0)) + ecum[r, :]
        m = cum[BL // 2 - 1 : BL // 2, :]
        last = cum[BL - 1 : BL, :]
        rel = cum - m
        ebuf[r, :] = jnp.exp2(rel)
        kd = (key * jnp.exp2(-rel)).astype(BF16)
        v = vbuf[r, :]
        for h in range(2):
            hc = slice(h * HK, (h + 1) * HK)
            kdiag[b, hc, hc] = kd[:, hc]
            vdiag[b, hc, hc] = v[:, hc]
        lpre = lrun[...]
        vecs[b, 0:1, :] = lpre
        vecs[b, 1:2, :] = m
        lrun[...] = lpre + last
        a = jnp.exp2(last)
        e2 = jnp.exp2(last - m)
        contrib = dot(v, kd, TN)
        for h in range(2):
            hc = slice(h * HK, (h + 1) * HK)
            s = run[h]
            sloc[b, h] = s
            run[h] = s * a[:, hc] + contrib[hc, hc] * e2[:, hc]

    def proj_p(i):
        r = pl.ds(i * OUT, OUT)
        o = dot(nbuf[r, :], wp[...]) * twice(rsbuf[r, :])
        pbuf[pl.ds(BL + i * OUT, OUT), :] = o.astype(BF16)

    def proj_qg(d):
        r = rows(d, OUT)
        n = nbuf[r, :]
        rs = twice(rsbuf[r, :])
        qbuf[r, :] = (silu(dot(n, wq[...]) * rs) * ebuf[r, :]).astype(BF16)
        gbuf[r, :] = silu(dot(n, wg[...]) * rs) * rgain[...]

    def score_block(b):
        r = rows(b, BL)
        s = dot(qbuf[r, :], kdiag[b], NT)
        s = jnp.where(twice(trilb[...]) > 0, s, 0.0).astype(BF16)
        winbuf[r, :] = dot(s, vdiag[b])

    def pool_rows(d):
        parts = []
        for s in range(3):
            b = d * 3 + s
            ext = pbuf[pl.ds(pl.multiple_of(b * BL, BL), 2 * BL), :]
            sums = dot(band[...], ext)
            t = sp * ROWS + b * BL + lax.broadcasted_iota(jnp.int32, (BL, 1), 0)
            cnt = jnp.minimum(t + 1, w).astype(F32)
            parts.append((sums * (1.0 / cnt) - ext[BL:, :].astype(F32)).astype(BF16))
        return (dot(jnp.concatenate(parts, axis=0), mix[0]) * pscale[...]).astype(BF16)

    def out_block(b):
        r = rows(b, BL)
        lpre = vecs[b, 0:1, :]
        m = vecs[b, 1:2, :]
        em = jnp.exp2(m)
        elm = jnp.exp2(lpre + m)
        st = [
            (sloc[b, h] * em[:, h * HK : (h + 1) * HK] + carr[h] * elm[:, h * HK : (h + 1) * HK]).astype(BF16)
            for h in range(2)
        ]
        o = winbuf[r, :] + dot(qbuf[r, :], diag2(st[0], st[1]), NT)
        g = gbuf[r, :]
        parts = []
        for h in range(2):
            hc = slice(h * HK, (h + 1) * HK)
            oh = o[:, hc]
            ms = jnp.sum(oh * oh, axis=-1, keepdims=True) * (1.0 / HK)
            parts.append(oh * lax.rsqrt(ms + EPS) * g[:, hc])
        return jnp.concatenate(parts, axis=1).astype(BF16)

    def chain(ea, eS, la, lS):
        return ea * la, la * eS + lS

    def put_state(ref, a, S):
        hi = a.astype(BF16)
        lo = (a - hi.astype(F32)).astype(BF16)
        ref[0:HK, :] = S.astype(BF16)
        ref[HK : HK + 8, :] = jnp.broadcast_to(hi, (8, HK))
        ref[HK + 8 : HK + 16, :] = jnp.broadcast_to(lo, (8, HK))

    def scan_states(ref, me):
        ta = jnp.ones((1, HK), F32)
        tS = jnp.zeros((HK, HK), F32)
        ea, eS = ta, tS
        for j in range(4):
            full = ref[j].astype(F32)
            ta, tS = chain(ta, tS, full[HK : HK + 1, :] + full[HK + 8 : HK + 9, :], full[0:HK, :])
            ea = jnp.where(me > j, ta, ea)
            eS = jnp.where(me > j, tS, eS)
        return ta, tS, ea, eS

    w1, w1f, w2, w2f, w3 = {}, {}, {}, {}, {}

    def shard_of(k):
        return lax.rem(x + 4 - k, 4)

    def piece(k, a, at, half=None):
        start = shard_of(k) * 256 + a * 128 + at * 32
        if half is None:
            return wout.at[c, pl.ds(pl.multiple_of(start, 32), 32)]
        return wout.at[c, pl.ds(pl.multiple_of(start + half * 16, 16), 16)]

    def mine(a):
        return z if a else y

    def w1_send():
        for a in (1, 0):
            for k in (1, 3):
                w1[k, a] = remote(
                    wst.at[c, a], piece(0, a, mine(a)), w1s.at[k // 2, a], w1r.at[k // 2, a], xpeer(k)
                )

    def w2_first(k, a):
        for q in (1, 3):
            sl = piece(k, a, mine(a))
            to = (zpeer if a else ypeer)(q)
            w2[k, a, q] = remote(sl, sl, w2s.at[a, k - 1, q // 2], w2r.at[a, k - 1, q // 2], to)

    def w1_poll(k, a):
        w1[k, a].wait_recv()
        h = k // 2
        sl = piece(k, a, mine(a), h)
        w1f[h, a] = remote(sl, sl, w1fs.at[h, a], w1fr.at[h, a], xpeer(k))
        w2_first(k, a)

    def w1_poll2(a):
        for h in range(2):
            w1f[h, a].wait_recv()
        w2_first(2, a)

    def w2_poll(k, a):
        for h, q in enumerate((1, 3)):
            w2[k, a, q].wait_recv()
            sl = piece(k, a, lax.rem(mine(a) + 4 - q, 4), h)
            to = (zpeer if a else ypeer)(q)
            w2f[k, a, h] = remote(sl, sl, w2fs.at[a, k - 1, h], w2fr.at[a, k - 1, h], to)
        for q in (0, 1, 3):
            w3_send(k, a, q)

    def w3_send(k, a, q):
        sl = piece(k, a, lax.rem(mine(a) + q, 4))
        w3[k, a, q] = remote(sl, sl, w3s.at[a, k - 1, q], w3r.at[a, k - 1, q], sib)

    def w3_poll(k, a):
        for h in range(2):
            w2f[k, a, h].wait_recv()
        w3_send(k, a, 2)

    r_i = lax.broadcasted_iota(jnp.int32, (BL, BL), 0)
    c_i = lax.broadcasted_iota(jnp.int32, (BL, BL), 1)
    trilb[...] = jnp.where(c_i <= r_i, 1.0, 0.0).astype(BF16)
    w = lax.shift_left(jnp.int32(2), x)
    r_w = lax.broadcasted_iota(jnp.int32, (BL, 2 * BL), 0)
    c_w = lax.broadcasted_iota(jnp.int32, (BL, 2 * BL), 1)
    diff = r_w + BL - c_w
    band[...] = jnp.where((diff >= 0) & (diff < w), 1.0, 0.0).astype(BF16)
    run[...] = jnp.zeros_like(run)
    lrun[...] = jnp.zeros_like(lrun)
    pbuf[pl.ds(0, BL - 16), :] = jnp.zeros((BL - 16, C), BF16)
    for b in range(NB):
        for h in range(2):
            hc, oc = slice(h * HK, (h + 1) * HK), slice((1 - h) * HK, (2 - h) * HK)
            kdiag[b, hc, oc] = jnp.zeros((HK, HK), BF16)
            vdiag[b, hc, oc] = jnp.zeros((HK, HK), BF16)
    l_extra.wait()
    for b in range(NB):
        extra_sums(b)

    l_gain.wait()
    l_x[0].wait()
    norm(0)
    l_wf.wait()
    l_wv.wait()
    l_lb.wait()
    for i in range(2, 4):
        l_x.append(load(x_hbm.at[pl.ds(i * OUT, OUT)], xbuf.at[pl.ds(i * OUT, OUT)]))
    l_p = load(wp_hbm, wp)
    l_q = load(wq_hbm, wq)
    l_g = load(wg_hbm, wg)
    l_init = load(init_hbm, init)
    l_rg = load(rgain_hbm, rgain)
    l_ps = load(pscale_hbm, pscale)
    l_mix = load(mix_hbm, mix)
    l_op = load(op_hbm, wout.at[0, rows(x, 256)])
    l_or = load(or_hbm, wout.at[1, rows(x, 256)])
    for i in range(4):
        if i < 3:
            l_x[i + 1].wait()
        proj_fv(i)
        if i < 3:
            norm(i + 1)
        if i > 0:
            for s in range(3):
                state_block(3 * i - 3 + s)
        if i == 0:
            for cp in l_pc:
                cp.wait()
            pl.semaphore_wait(bar, jnp.where((sp == 0) | (sp == 31), 11, 12))
            w1_send()
    for s in range(3):
        state_block(9 + s)

    for h in range(2):
        totsend[h, 0:HK, :] = run[h]
        al = jnp.exp2(lrun[:, h * HK : (h + 1) * HK])
        totsend[h, HK : HK + 8, :] = jnp.broadcast_to(al, (8, HK))
    e_cp = remote(totsend, totrecv, es, er, sib)

    l_p.wait()
    proj_p(3)
    proj_p(0)
    h_cp = remote(pbuf.at[pl.ds(BL + ROWS - 16, 16)], pbuf.at[pl.ds(BL - 16, 16)], hs, hr, nxt, False)

    @pl.when(sp < 31)
    def _():
        h_cp.start()

    w1_poll(1, 1)
    w1_poll(3, 1)
    e_cp.wait()
    oS, oa = totsend[c, 0:HK, :], totsend[c, HK : HK + 1, :]
    sS, sa = totrecv[c, 0:HK, :], totrecv[c, HK : HK + 1, :]
    first = c == 0
    ea, eS = jnp.where(first, oa, sa), jnp.where(first, oS, sS)
    la, lS = jnp.where(first, sa, oa), jnp.where(first, sS, oS)
    put_state(ybuf.at[y], *chain(ea, eS, la, lS))
    y_cp = [
        remote(ybuf.at[y], ybuf.at[y], ys.at[k - 1], yr_.at[k - 1], ypeer(k)) for k in (2, 1, 3)
    ]
    w1_poll(1, 0)
    w1_poll(3, 0)
    proj_p(1)
    proj_p(2)
    l_ps.wait()
    l_mix.wait()
    @pl.when(sp < 31)
    def _():
        h_cp.wait_send()

    @pl.when(sp > 0)
    def _():
        h_cp.wait_recv()

    @pl.when(sp == 0)
    def _():
        pbuf[pl.ds(BL - 16, 16), :] = jnp.zeros((16, C), BF16)

    ap = {}

    def do_pool(ks):
        blks = [pool_rows(lax.rem(x + k, 4)) for k in ks]
        for k, blk in zip(ks, blks):
            if k:
                ypbuf[k - 1] = blk
            else:
                ypseen[x] = blk
        for k in ks:
            if k:
                ap[k] = remote(ypbuf.at[k - 1], ypseen.at[x], aps.at[k - 1], apr.at[k - 1], xpeer(k))

    do_pool((1, 3))
    do_pool((2, 0))

    def do_proj(k):
        proj_qg(lax.rem(x + k, 4))

    def do_scores(k):
        for s in range(3):
            score_block(lax.rem(x + k, 4) * 3 + s)

    def do_qg(k):
        do_proj(k)
        do_scores(k)

    ar = {}

    def do_out(ks):
        blks = [[out_block(lax.rem(x + k, 4) * 3 + s) for s in range(3)] for k in ks]
        for k, blk in zip(ks, blks):
            for s in range(3):
                if k:
                    yrbuf[k - 1, pl.ds(s * BL, BL), :] = blk[s]
                else:
                    yrseen[x, pl.ds(s * BL, BL), :] = blk[s]
        for k in ks:
            if k:
                ar[k] = remote(yrbuf.at[k - 1], yrseen.at[x], ars.at[k - 1], arr.at[k - 1], xpeer(k))

    l_q.wait()
    l_g.wait()
    l_rg.wait()
    do_proj(1)
    for cp in y_cp:
        cp.wait()
    ta, tS, ya, yS = scan_states(ybuf, y)
    put_state(zbuf.at[z], ta, tS)
    pst[0:HK, :] = yS
    pst[HK : HK + 8, :] = jnp.broadcast_to(ya, (8, HK))
    z_cp = {
        k: remote(zbuf.at[z], zbuf.at[z], zs.at[k - 1], zr.at[k - 1], zpeer(k), False) for k in (2, 1, 3)
    }
    for k, cp in z_cp.items():
        pl.when(z + k < 4)(cp.start)
    do_scores(1)
    do_qg(3)
    w1_poll2(0)
    w1_poll2(1)
    do_proj(2)
    for k, cp in z_cp.items():
        pl.when(z >= k)(cp.wait_recv)
    ta, tS, za, zS = scan_states(zbuf, z)
    l_init.wait()
    fa, fS = chain(za, zS, pst[HK : HK + 1, :], pst[0:HK, :])
    carr[c] = fa * jnp.transpose(init[c]) + fS
    c_cp = remote(carr.at[c], carr.at[c], cs, cr, sib)
    do_scores(2)
    w2_poll(1, 1)
    w2_poll(1, 0)
    w2_poll(3, 1)
    c_cp.wait()
    for h in range(2):
        cur = carr[h]
        later = totrecv[h, HK : HK + 1, :] * cur + totrecv[h, 0:HK, :]
        carr[h] = jnp.where(c == 0, cur, later)
    do_out((1, 3))
    do_out((2,))
    w2_poll(3, 0)
    do_qg(0)
    w2_poll(2, 1)
    w2_poll(2, 0)
    do_out((0,))
    w3_poll(1, 1)
    w3_poll(1, 0)
    w3_poll(3, 1)
    l_op.wait()
    l_or.wait()

    def out_dot(parts, nc):
        left = [(yrseen if mat else ypseen)[shard_of(k)] for mat, k in parts]
        right = [wout[mat, rows(shard_of(k), 256), nc] for mat, k in parts]
        return dot(jnp.concatenate(left, axis=1), jnp.concatenate(right, axis=0))

    for n in range(4):
        nc = pl.ds(n * 512, 512)
        acc[:, nc] = out_dot(((0, 0), (1, 0)), nc)
    w3_poll(3, 0)
    w3_poll(2, 1)
    w3_poll(2, 0)
    for cp in ap.values():
        cp.wait()
    for cp in w3.values():
        cp.wait()
    for n in range(4):
        nc = pl.ds(n * 512, 512)
        acc[:, nc] += out_dot(((0, 1), (0, 3), (0, 2)), nc)
    ar[1].wait()
    ar[3].wait()
    for n in range(4):
        nc = pl.ds(n * 512, 512)
        acc[:, nc] += out_dot(((1, 1), (1, 3)), nc)
    ar[2].wait()
    outs = []
    for n in range(4):
        nc = pl.ds(n * 512, 512)
        obuf[n] = (acc[:, nc] + out_dot(((1, 2),), nc)).astype(BF16)
        cp = pltpu.make_async_copy(obuf.at[n], out_ref.at[:, nc], osem.at[n])
        cp.start()
        outs.append(cp)
    for k, cp in z_cp.items():
        pl.when(z + k < 4)(cp.wait_send)
    for group in (w1, w1f, w2, w2f):
        for cp in group.values():
            cp.wait_send()
    for cp in outs:
        cp.wait()


def copy_out(src, dst, buf, sin, sout):
    n = OUT // 4
    into = [pltpu.make_async_copy(src.at[pl.ds(i * n, n)], buf.at[i], sin.at[i]) for i in range(4)]
    out = [pltpu.make_async_copy(buf.at[i], dst.at[pl.ds(i * n, n)], sout.at[i]) for i in range(4)]
    for cp in into:
        cp.start()
    for cp, to in zip(into, out):
        cp.wait()
        to.start()
    for to in out:
        to.wait()


def scratch():
    V = pltpu.VMEM
    S = pltpu.SemaphoreType.DMA
    return [
        V((ROWS, D), BF16), V((ROWS, D), BF16), V((D, C), BF16), V((D, C), BF16), V((D, C), BF16),
        V((D, C), BF16), V((D, C), BF16),         V((2, 2, 32, D), BF16), V((2, 4 * C, D), BF16),
        V((1, D), F32), V((1, C), F32), V((1, C), F32), V((1, C), F32),
        V((2, ROWS), F32), V((1, C, C), BF16), V((2, HK, HK), F32),
        V((ROWS, HK), F32), V((ROWS, C), F32), V((ROWS, C), F32), V((ROWS, C), BF16), V((ROWS, C), F32),
        V((NB, C, C), BF16), V((NB, C, C), BF16), V((ROWS, C), BF16), V((ROWS, C), F32), V((ROWS, C), F32),
        V((BL + ROWS, C), BF16), V((NB, 2, HK, HK), F32), V((2, HK, HK), F32), V((1, C), F32), V((NB, 2, C), F32),
        V((2, HK + 8, HK), F32), V((2, HK + 8, HK), F32), V((4, PF, HK), BF16), V((4, PF, HK), BF16), V((HK + 8, HK), F32), V((2, HK, HK), F32),
        V((BL, BL), BF16), V((BL, 2 * BL), BF16),
        V((3, OUT, C), BF16), V((4, OUT, C), BF16), V((3, OUT, C), BF16), V((4, OUT, C), BF16),
        V((OUT, D), F32), V((4, OUT, 512), BF16),
        S((24,)), S((2, 2)), S((2, 2)), S((2, 2)), S((2, 2)), S((2, 3, 2)), S((2, 3, 2)), S((2, 3, 2)), S((2, 3, 2)),
        S((2, 3, 4)), S((2, 3, 4)),
        S(()), S(()), S((3,)), S((3,)), S((3,)), S((3,)), S(()), S(()), S(()), S(()), S((3,)), S((3,)), S((3,)), S((3,)),
        S((4,)),
    ]


def per_device(
    inputs, norm_gain, pool_weight, query_weight, forget_weight, value_weight, outgate_weight,
    pool_mix, pool_scale, lower_bound, extra_decay, recur_gain, init_state, out_pool, out_recur,
):
    anyspec = pl.BlockSpec(memory_space=pl.ANY)
    full = pl.pallas_call(
        kernel,
        out_shape=jax.ShapeDtypeStruct((OUT, D), BF16),
        in_specs=[anyspec] * 15,
        out_specs=anyspec,
        scratch_shapes=scratch(),
        compiler_params=pltpu.CompilerParams(
            collective_id=0, has_side_effects=True, vmem_limit_bytes=63 * 1024 * 1024
        ),
    )(
        inputs, norm_gain.reshape(1, D), pool_weight, query_weight, forget_weight, value_weight,
        outgate_weight, pool_mix, pool_scale.reshape(1, C), lower_bound.reshape(1, C),
        extra_decay.T, recur_gain.reshape(1, C), init_state, out_pool, out_recur,
    )
    return pl.pallas_call(
        copy_out,
        out_shape=jax.ShapeDtypeStruct((OUT, D), BF16),
        in_specs=[anyspec],
        out_specs=anyspec,
        scratch_shapes=[
            pltpu.VMEM((4, OUT // 4, D), BF16), pltpu.SemaphoreType.DMA((4,)), pltpu.SemaphoreType.DMA((4,)),
        ],
    )(full)


def solution(mesh):
    placed = (
        P("sp", None), P(), P(None, "tp"), P(None, "tp"), P(None, "tp"), P(None, "tp"), P(None, "tp"),
        P("tp", None, None), P("tp"), P("tp"), P("sp", "tp"), P("tp"), P("tp", None, None),
        P("tp", None), P("tp", None),
    )
    return jax.shard_map(
        per_device, mesh=mesh, in_specs=placed, out_specs=P(("sp", "tp"), None), check_vma=False
    )
```

```python
import jax
import jax.numpy as jnp
from jax import lax
from jax.experimental import pallas as pl
from jax.experimental.pallas import tpu as pltpu
from jax.sharding import PartitionSpec as P

MESH = pl.DeviceIdType.MESH
F32 = jnp.float32
BF16 = jnp.bfloat16
EPS = 1e-5

ROWS = 1536
OUT = 384
BL = 128
NB = ROWS // BL
C = 256
HK = 128
D = 2048
PF = HK + 16

NT = (((1,), (1,)), ((), ()))
TN = (((0,), (0,)), ((), ()))
NN = (((1,), (0,)), ((), ()))

LOG2E = 1.4426950408889634
POLY = (-LOG2E, -0.7213472908955184, -0.48097089760573397, -0.3571200043786398, -0.3431147843908393)


def dot(a, b, dims=NN):
    return lax.dot_general(a, b, dims, preferred_element_type=F32)


def silu(v):
    half = 0.5 * v
    return half + half * jnp.tanh(half)


def twice(a):
    return jnp.concatenate([a, a], axis=1)


def diag2(a, b):
    zero = jnp.zeros((HK, HK), BF16)
    top = jnp.concatenate([a, zero], axis=1)
    return jnp.concatenate([top, jnp.concatenate([zero, b], axis=1)], axis=0)


def kernel(
    x_hbm, gain_hbm, wp_hbm, wq_hbm, wf_hbm, wv_hbm, wg_hbm, mix_hbm, pscale_hbm, lb_hbm,
    extra_hbm, rgain_hbm, init_hbm, op_hbm, or_hbm,
    out_ref,
    xbuf, nbuf, wf, wv, wq, wg, wp, wst, wout, gain, pscale, lb, rgain, extra, mix, init,
    rsbuf, ecum, fbuf, vbuf, ebuf, kdiag, vdiag, qbuf, winbuf, gbuf, pbuf, sloc, run, lrun, vecs,
    totsend, totrecv, ybuf, zbuf, pst, carr, trilb, band,
    ypbuf, ypseen, yrbuf, yrseen, acc, obuf,
    lsem, w1s, w1r, w1fs, w1fr, w2s, w2r, w2fs, w2fr, w3s, w3r,
    es, er, ys, yr_, zs, zr, cs, cr, hs, hr, aps, apr, ars, arr, osem,
):
    x = lax.axis_index("tp")
    sp = lax.axis_index("sp")
    c = lax.rem(sp, 2)
    chip = lax.div(sp, 2)
    y = lax.rem(chip, 4)
    z = lax.div(chip, 4)

    def dev(spi, tpi):
        return {"sp": spi, "tp": tpi}

    def xpeer(k):
        return dev(sp, lax.rem(x + k, 4))

    def ypeer(k):
        return dev(z * 8 + lax.rem(y + k, 4) * 2 + c, x)

    def zpeer(k):
        return dev(lax.rem(z + k, 4) * 8 + y * 2 + c, x)

    sib = dev(sp + 1 - 2 * c, x)
    nxt = dev(lax.rem(sp + 1, 32), x)
    prv = dev(lax.rem(sp + 31, 32), x)

    count = [0]

    def load(src, dst):
        i = count[0]
        count[0] += 1
        cp = pltpu.make_async_copy(src, dst, lsem.at[i])
        cp.start()
        return cp

    def remote(src, dst, ssem, rsem, to, start=True):
        cp = pltpu.make_async_remote_copy(
            src_ref=src, dst_ref=dst, send_sem=ssem, recv_sem=rsem, device_id=to, device_id_type=MESH
        )
        if start:
            cp.start()
        return cp

    def rows(i, n):
        return pl.ds(pl.multiple_of(i * n, n), n)

    pa = pl.multiple_of(y * 32, 32)
    pb = pl.multiple_of(128 + z * 32, 32)
    l_extra = load(extra_hbm, extra)
    l_gain = load(gain_hbm, gain)
    l_x = [load(x_hbm.at[pl.ds(0, OUT)], xbuf.at[pl.ds(0, OUT)])]
    l_wf = load(wf_hbm, wf)
    l_wv = load(wv_hbm, wv)
    l_lb = load(lb_hbm, lb)
    bar = pltpu.get_barrier_semaphore()
    for k in (1, 2, 3):
        for peer in (xpeer, ypeer, zpeer):
            pl.semaphore_signal(bar, inc=1, device_id=peer(k), device_id_type=MESH)
    pl.semaphore_signal(bar, inc=1, device_id=sib, device_id_type=MESH)

    @pl.when(sp < 31)
    def _():
        pl.semaphore_signal(bar, inc=1, device_id=nxt, device_id_type=MESH)

    @pl.when(sp > 0)
    def _():
        pl.semaphore_signal(bar, inc=1, device_id=prv, device_id_type=MESH)


    def extra_sums(b):
        parts = []
        for h in range(2):
            e = extra[h : h + 1, b * BL : (b + 1) * BL] * LOG2E
            hi = e.astype(BF16)
            lo = (e - hi.astype(F32)).astype(BF16)
            t = trilb[...]
            parts.append(jnp.concatenate([t * hi, t * lo], axis=1))
        o = dot(jnp.concatenate(parts, axis=0), jnp.ones((2 * BL, HK), BF16))
        r = pl.ds(b * BL, BL)
        ecum[r, 0:HK] = o[:BL]
        ecum[r, HK:] = o[BL:]

    def norm(j):
        g = gain[...].astype(BF16)
        sums = []
        for s in range(3):
            r = pl.ds(j * OUT + s * BL, BL)
            v = xbuf[r, :]
            nbuf[r, :] = v * g
            sq = v * v
            t = [sq[:, i * 256 : (i + 1) * 256] for i in range(8)]
            while len(t) > 1:
                t = [t[i] + t[i + 1] for i in range(0, len(t), 2)]
            sums.append(t[0])
        ss = dot(jnp.concatenate(sums, axis=0), jnp.ones((256, HK), BF16))
        rsbuf[pl.ds(j * OUT, OUT), :] = lax.rsqrt(ss * (1.0 / D) + EPS)

    def proj_fv(j):
        r = pl.ds(j * OUT, OUT)
        n = nbuf[r, :]
        rs = twice(rsbuf[r, :])
        fbuf[r, :] = dot(n, wf[...]) * (0.5 * rs)
        vbuf[r, :] = (dot(n, wv[...]) * rs).astype(BF16)

    def state_block(b):
        r = pl.ds(b * BL, BL)
        half = 0.5 * (1.0 - lb[...])
        key = half - half * jnp.tanh(fbuf[r, :])
        lf = POLY[4] * key + POLY[3]
        for n in (2, 1, 0):
            lf = lf * key + POLY[n]
        lf = lf * key
        hi = lf.astype(BF16)
        lo = (lf - hi.astype(F32)).astype(BF16)
        t = trilb[...]
        cum = dot(twice(t), jnp.concatenate([hi, lo], axis=0)) + ecum[r, :]
        m = cum[BL // 2 - 1 : BL // 2, :]
        last = cum[BL - 1 : BL, :]
        rel = cum - m
        ebuf[r, :] = jnp.exp2(rel)
        kd = (key * jnp.exp2(-rel)).astype(BF16)
        v = vbuf[r, :]
        for h in range(2):
            hc = slice(h * HK, (h + 1) * HK)
            kdiag[b, hc, hc] = kd[:, hc]
            vdiag[b, hc, hc] = v[:, hc]
        lpre = lrun[...]
        vecs[b, 0:1, :] = lpre
        vecs[b, 1:2, :] = m
        lrun[...] = lpre + last
        a = jnp.exp2(last)
        e2 = jnp.exp2(last - m)
        contrib = dot(v, kd, TN)
        for h in range(2):
            hc = slice(h * HK, (h + 1) * HK)
            s = run[h]
            sloc[b, h] = s
            run[h] = s * a[:, hc] + contrib[hc, hc] * e2[:, hc]

    def proj_p(i):
        r = pl.ds(i * OUT, OUT)
        o = dot(nbuf[r, :], wp[...]) * twice(rsbuf[r, :])
        pbuf[pl.ds(BL + i * OUT, OUT), :] = o.astype(BF16)

    def proj_qg(d):
        r = rows(d, OUT)
        n = nbuf[r, :]
        rs = twice(rsbuf[r, :])
        qbuf[r, :] = (silu(dot(n, wq[...]) * rs) * ebuf[r, :]).astype(BF16)
        gbuf[r, :] = silu(dot(n, wg[...]) * rs) * rgain[...]

    def score_block(b):
        r = rows(b, BL)
        s = dot(qbuf[r, :], kdiag[b], NT)
        s = jnp.where(twice(trilb[...]) > 0, s, 0.0).astype(BF16)
        winbuf[r, :] = dot(s, vdiag[b])

    def pool_rows(d):
        parts = []
        for s in range(3):
            b = d * 3 + s
            ext = pbuf[pl.ds(pl.multiple_of(b * BL, BL), 2 * BL), :]
            sums = dot(band[...], ext)
            t = sp * ROWS + b * BL + lax.broadcasted_iota(jnp.int32, (BL, 1), 0)
            cnt = jnp.minimum(t + 1, w).astype(F32)
            parts.append((sums * (1.0 / cnt) - ext[BL:, :].astype(F32)).astype(BF16))
        return (dot(jnp.concatenate(parts, axis=0), mix[0]) * pscale[...]).astype(BF16)

    def out_block(b):
        r = rows(b, BL)
        lpre = vecs[b, 0:1, :]
        m = vecs[b, 1:2, :]
        em = jnp.exp2(m)
        elm = jnp.exp2(lpre + m)
        st = [
            (sloc[b, h] * em[:, h * HK : (h + 1) * HK] + carr[h] * elm[:, h * HK : (h + 1) * HK]).astype(BF16)
            for h in range(2)
        ]
        o = winbuf[r, :] + dot(qbuf[r, :], diag2(st[0], st[1]), NT)
        g = gbuf[r, :]
        parts = []
        for h in range(2):
            hc = slice(h * HK, (h + 1) * HK)
            oh = o[:, hc]
            ms = jnp.sum(oh * oh, axis=-1, keepdims=True) * (1.0 / HK)
            parts.append(oh * lax.rsqrt(ms + EPS) * g[:, hc])
        return jnp.concatenate(parts, axis=1).astype(BF16)

    def chain(ea, eS, la, lS):
        return ea * la, la * eS + lS

    def put_state(ref, a, S):
        hi = a.astype(BF16)
        lo = (a - hi.astype(F32)).astype(BF16)
        ref[0:HK, :] = S.astype(BF16)
        ref[HK : HK + 8, :] = jnp.broadcast_to(hi, (8, HK))
        ref[HK + 8 : HK + 16, :] = jnp.broadcast_to(lo, (8, HK))

    def scan_states(ref, me):
        ta = jnp.ones((1, HK), F32)
        tS = jnp.zeros((HK, HK), F32)
        ea, eS = ta, tS
        for j in range(4):
            full = ref[j].astype(F32)
            ta, tS = chain(ta, tS, full[HK : HK + 1, :] + full[HK + 8 : HK + 9, :], full[0:HK, :])
            ea = jnp.where(me > j, ta, ea)
            eS = jnp.where(me > j, tS, eS)
        return ta, tS, ea, eS

    w1, w1f, w2, w2f, w3 = {}, {}, {}, {}, {}

    def shard_of(k):
        return lax.rem(x + 4 - k, 4)

    def piece(k, a, at, half=None):
        start = shard_of(k) * 256 + a * 128 + at * 32
        if half is None:
            return wout.at[c, pl.ds(pl.multiple_of(start, 32), 32)]
        return wout.at[c, pl.ds(pl.multiple_of(start + half * 16, 16), 16)]

    def mine(a):
        return z if a else y

    def w1_send():
        for a in (1, 0):
            for k in (1, 3):
                w1[k, a] = remote(
                    wst.at[c, a], piece(0, a, mine(a)), w1s.at[k // 2, a], w1r.at[k // 2, a], xpeer(k)
                )

    def w2_first(k, a):
        for q in (1, 3):
            sl = piece(k, a, mine(a))
            to = (zpeer if a else ypeer)(q)
            w2[k, a, q] = remote(sl, sl, w2s.at[a, k - 1, q // 2], w2r.at[a, k - 1, q // 2], to)

    def w1_poll(k, a):
        w1[k, a].wait_recv()
        h = k // 2
        sl = piece(k, a, mine(a), h)
        w1f[h, a] = remote(sl, sl, w1fs.at[h, a], w1fr.at[h, a], xpeer(k))
        w2_first(k, a)

    def w1_poll2(a):
        for h in range(2):
            w1f[h, a].wait_recv()
        w2_first(2, a)

    def w2_poll(k, a):
        for h, q in enumerate((1, 3)):
            w2[k, a, q].wait_recv()
            sl = piece(k, a, lax.rem(mine(a) + 4 - q, 4), h)
            to = (zpeer if a else ypeer)(q)
            w2f[k, a, h] = remote(sl, sl, w2fs.at[a, k - 1, h], w2fr.at[a, k - 1, h], to)
        for q in (0, 1, 3):
            w3_send(k, a, q)

    def w3_send(k, a, q):
        sl = piece(k, a, lax.rem(mine(a) + q, 4))
        w3[k, a, q] = remote(sl, sl, w3s.at[a, k - 1, q], w3r.at[a, k - 1, q], sib)

    def w3_poll(k, a):
        for h in range(2):
            w2f[k, a, h].wait_recv()
        w3_send(k, a, 2)

    r_i = lax.broadcasted_iota(jnp.int32, (BL, BL), 0)
    c_i = lax.broadcasted_iota(jnp.int32, (BL, BL), 1)
    trilb[...] = jnp.where(c_i <= r_i, 1.0, 0.0).astype(BF16)
    w = lax.shift_left(jnp.int32(2), x)
    r_w = lax.broadcasted_iota(jnp.int32, (BL, 2 * BL), 0)
    c_w = lax.broadcasted_iota(jnp.int32, (BL, 2 * BL), 1)
    diff = r_w + BL - c_w
    band[...] = jnp.where((diff >= 0) & (diff < w), 1.0, 0.0).astype(BF16)
    run[...] = jnp.zeros_like(run)
    lrun[...] = jnp.zeros_like(lrun)
    pbuf[pl.ds(0, BL - 16), :] = jnp.zeros((BL - 16, C), BF16)
    for b in range(NB):
        for h in range(2):
            hc, oc = slice(h * HK, (h + 1) * HK), slice((1 - h) * HK, (2 - h) * HK)
            kdiag[b, hc, oc] = jnp.zeros((HK, HK), BF16)
            vdiag[b, hc, oc] = jnp.zeros((HK, HK), BF16)
    l_extra.wait()
    for b in range(NB):
        extra_sums(b)

    l_gain.wait()
    l_x[0].wait()
    norm(0)
    l_pc = [load(op_hbm.at[pl.ds(pa, 32)], wst.at[0, 0]), load(op_hbm.at[pl.ds(pb, 32)], wst.at[0, 1])]
    l_pc += [load(or_hbm.at[pl.ds(pa, 32)], wst.at[1, 0]), load(or_hbm.at[pl.ds(pb, 32)], wst.at[1, 1])]
    for i in range(1, 4):
        l_x.append(load(x_hbm.at[pl.ds(i * OUT, OUT)], xbuf.at[pl.ds(i * OUT, OUT)]))
    l_p = load(wp_hbm, wp)
    l_q = load(wq_hbm, wq)
    l_g = load(wg_hbm, wg)
    l_init = load(init_hbm, init)
    l_rg = load(rgain_hbm, rgain)
    l_ps = load(pscale_hbm, pscale)
    l_mix = load(mix_hbm, mix)
    l_op = load(op_hbm, wout.at[0, rows(x, 256)])
    l_or = load(or_hbm, wout.at[1, rows(x, 256)])
    l_wf.wait()
    l_wv.wait()
    l_lb.wait()
    proj_fv(0)
    for cp in l_pc:
        cp.wait()
    pl.semaphore_wait(bar, jnp.where((sp == 0) | (sp == 31), 11, 12))
    w1_send()
    l_x[1].wait()
    norm(1)
    l_x[2].wait()
    proj_fv(1)
    norm(2)
    for s in range(3):
        state_block(s)
    l_x[3].wait()
    proj_fv(2)
    norm(3)
    for s in range(3):
        state_block(3 + s)
    proj_fv(3)
    for s in range(3):
        state_block(6 + s)
    for s in range(3):
        state_block(9 + s)

    for h in range(2):
        totsend[h, 0:HK, :] = run[h]
        al = jnp.exp2(lrun[:, h * HK : (h + 1) * HK])
        totsend[h, HK : HK + 8, :] = jnp.broadcast_to(al, (8, HK))
    e_cp = remote(totsend, totrecv, es, er, sib)

    w1_poll(1, 1)
    w1_poll(3, 1)
    l_p.wait()
    proj_p(3)
    proj_p(0)
    h_cp = remote(pbuf.at[pl.ds(BL + ROWS - 16, 16)], pbuf.at[pl.ds(BL - 16, 16)], hs, hr, nxt, False)

    @pl.when(sp < 31)
    def _():
        h_cp.start()

    e_cp.wait()
    oS, oa = totsend[c, 0:HK, :], totsend[c, HK : HK + 1, :]
    sS, sa = totrecv[c, 0:HK, :], totrecv[c, HK : HK + 1, :]
    first = c == 0
    ea, eS = jnp.where(first, oa, sa), jnp.where(first, oS, sS)
    la, lS = jnp.where(first, sa, oa), jnp.where(first, sS, oS)
    put_state(ybuf.at[y], *chain(ea, eS, la, lS))
    y_cp = [
        remote(ybuf.at[y], ybuf.at[y], ys.at[k - 1], yr_.at[k - 1], ypeer(k)) for k in (2, 1, 3)
    ]
    proj_p(1)
    proj_p(2)
    l_ps.wait()
    l_mix.wait()
    w1_poll(1, 0)
    w1_poll(3, 0)
    @pl.when(sp < 31)
    def _():
        h_cp.wait_send()

    @pl.when(sp > 0)
    def _():
        h_cp.wait_recv()

    @pl.when(sp == 0)
    def _():
        pbuf[pl.ds(BL - 16, 16), :] = jnp.zeros((16, C), BF16)

    ap = {}

    def do_pool(ks):
        blks = [pool_rows(lax.rem(x + k, 4)) for k in ks]
        for k, blk in zip(ks, blks):
            if k:
                ypbuf[k - 1] = blk
            else:
                ypseen[x] = blk
        for k in ks:
            if k:
                ap[k] = remote(ypbuf.at[k - 1], ypseen.at[x], aps.at[k - 1], apr.at[k - 1], xpeer(k))

    do_pool((1, 3))
    do_pool((2, 0))

    def do_proj(k):
        proj_qg(lax.rem(x + k, 4))

    def do_scores(k):
        for s in range(3):
            score_block(lax.rem(x + k, 4) * 3 + s)

    def do_qg(k):
        do_proj(k)
        do_scores(k)

    ar = {}

    def do_out(ks):
        blks = [[out_block(lax.rem(x + k, 4) * 3 + s) for s in range(3)] for k in ks]
        for k, blk in zip(ks, blks):
            for s in range(3):
                if k:
                    yrbuf[k - 1, pl.ds(s * BL, BL), :] = blk[s]
                else:
                    yrseen[x, pl.ds(s * BL, BL), :] = blk[s]
        for k in ks:
            if k:
                ar[k] = remote(yrbuf.at[k - 1], yrseen.at[x], ars.at[k - 1], arr.at[k - 1], xpeer(k))

    l_q.wait()
    l_g.wait()
    l_rg.wait()
    do_proj(1)
    for cp in y_cp:
        cp.wait()
    ta, tS, ya, yS = scan_states(ybuf, y)
    put_state(zbuf.at[z], ta, tS)
    pst[0:HK, :] = yS
    pst[HK : HK + 8, :] = jnp.broadcast_to(ya, (8, HK))
    z_cp = {
        k: remote(zbuf.at[z], zbuf.at[z], zs.at[k - 1], zr.at[k - 1], zpeer(k), False) for k in (2, 1, 3)
    }
    for k, cp in z_cp.items():
        pl.when(z + k < 4)(cp.start)
    w1_poll2(1)
    do_scores(1)
    w1_poll2(0)
    do_qg(3)
    w2_poll(1, 1)
    w2_poll(3, 1)
    do_proj(2)
    for k, cp in z_cp.items():
        pl.when(z >= k)(cp.wait_recv)
    ta, tS, za, zS = scan_states(zbuf, z)
    l_init.wait()
    fa, fS = chain(za, zS, pst[HK : HK + 1, :], pst[0:HK, :])
    carr[c] = fa * jnp.transpose(init[c]) + fS
    c_cp = remote(carr.at[c], carr.at[c], cs, cr, sib)
    do_scores(2)
    w2_poll(1, 0)
    w2_poll(3, 0)
    c_cp.wait()
    for h in range(2):
        cur = carr[h]
        later = totrecv[h, HK : HK + 1, :] * cur + totrecv[h, 0:HK, :]
        carr[h] = jnp.where(c == 0, cur, later)
    do_out((1, 3))
    do_out((2,))
    w2_poll(2, 1)
    do_proj(0)
    w2_poll(2, 0)
    do_scores(0)
    do_out((0,))
    w3_poll(1, 1)
    w3_poll(1, 0)
    w3_poll(3, 1)
    l_op.wait()
    l_or.wait()

    def out_dot(parts, nc):
        left = [(yrseen if mat else ypseen)[shard_of(k)] for mat, k in parts]
        right = [wout[mat, rows(shard_of(k), 256), nc] for mat, k in parts]
        return dot(jnp.concatenate(left, axis=1), jnp.concatenate(right, axis=0))

    for n in range(4):
        nc = pl.ds(n * 512, 512)
        acc[:, nc] = out_dot(((0, 0), (1, 0)), nc)
    w3_poll(3, 0)
    w3_poll(2, 1)
    w3_poll(2, 0)
    for cp in ap.values():
        cp.wait()
    for cp in w3.values():
        cp.wait()
    for n in range(4):
        nc = pl.ds(n * 512, 512)
        acc[:, nc] += out_dot(((0, 1), (0, 3), (0, 2)), nc)
    ar[1].wait()
    ar[3].wait()
    for n in range(4):
        nc = pl.ds(n * 512, 512)
        acc[:, nc] += out_dot(((1, 1), (1, 3)), nc)
    ar[2].wait()
    outs = []
    for n in range(4):
        nc = pl.ds(n * 512, 512)
        obuf[n] = (acc[:, nc] + out_dot(((1, 2),), nc)).astype(BF16)
        cp = pltpu.make_async_copy(obuf.at[n], out_ref.at[:, nc], osem.at[n])
        cp.start()
        outs.append(cp)
    for k, cp in z_cp.items():
        pl.when(z + k < 4)(cp.wait_send)
    for group in (w1, w1f, w2, w2f):
        for cp in group.values():
            cp.wait_send()
    for cp in outs:
        cp.wait()


def copy_out(src, dst, buf, sin, sout):
    n = OUT // 4
    into = [pltpu.make_async_copy(src.at[pl.ds(i * n, n)], buf.at[i], sin.at[i]) for i in range(4)]
    out = [pltpu.make_async_copy(buf.at[i], dst.at[pl.ds(i * n, n)], sout.at[i]) for i in range(4)]
    for cp in into:
        cp.start()
    for cp, to in zip(into, out):
        cp.wait()
        to.start()
    for to in out:
        to.wait()


def scratch():
    V = pltpu.VMEM
    S = pltpu.SemaphoreType.DMA
    return [
        V((ROWS, D), BF16), V((ROWS, D), BF16), V((D, C), BF16), V((D, C), BF16), V((D, C), BF16),
        V((D, C), BF16), V((D, C), BF16),         V((2, 2, 32, D), BF16), V((2, 4 * C, D), BF16),
        V((1, D), F32), V((1, C), F32), V((1, C), F32), V((1, C), F32),
        V((2, ROWS), F32), V((1, C, C), BF16), V((2, HK, HK), F32),
        V((ROWS, HK), F32), V((ROWS, C), F32), V((ROWS, C), F32), V((ROWS, C), BF16), V((ROWS, C), F32),
        V((NB, C, C), BF16), V((NB, C, C), BF16), V((ROWS, C), BF16), V((ROWS, C), F32), V((ROWS, C), F32),
        V((BL + ROWS, C), BF16), V((NB, 2, HK, HK), F32), V((2, HK, HK), F32), V((1, C), F32), V((NB, 2, C), F32),
        V((2, HK + 8, HK), F32), V((2, HK + 8, HK), F32), V((4, PF, HK), BF16), V((4, PF, HK), BF16), V((HK + 8, HK), F32), V((2, HK, HK), F32),
        V((BL, BL), BF16), V((BL, 2 * BL), BF16),
        V((3, OUT, C), BF16), V((4, OUT, C), BF16), V((3, OUT, C), BF16), V((4, OUT, C), BF16),
        V((OUT, D), F32), V((4, OUT, 512), BF16),
        S((24,)), S((2, 2)), S((2, 2)), S((2, 2)), S((2, 2)), S((2, 3, 2)), S((2, 3, 2)), S((2, 3, 2)), S((2, 3, 2)),
        S((2, 3, 4)), S((2, 3, 4)),
        S(()), S(()), S((3,)), S((3,)), S((3,)), S((3,)), S(()), S(()), S(()), S(()), S((3,)), S((3,)), S((3,)), S((3,)),
        S((4,)),
    ]


def per_device(
    inputs, norm_gain, pool_weight, query_weight, forget_weight, value_weight, outgate_weight,
    pool_mix, pool_scale, lower_bound, extra_decay, recur_gain, init_state, out_pool, out_recur,
):
    anyspec = pl.BlockSpec(memory_space=pl.ANY)
    full = pl.pallas_call(
        kernel,
        out_shape=jax.ShapeDtypeStruct((OUT, D), BF16),
        in_specs=[anyspec] * 15,
        out_specs=anyspec,
        scratch_shapes=scratch(),
        compiler_params=pltpu.CompilerParams(
            collective_id=0, has_side_effects=True, vmem_limit_bytes=63 * 1024 * 1024
        ),
    )(
        inputs, norm_gain.reshape(1, D), pool_weight, query_weight, forget_weight, value_weight,
        outgate_weight, pool_mix, pool_scale.reshape(1, C), lower_bound.reshape(1, C),
        extra_decay.T, recur_gain.reshape(1, C), init_state, out_pool, out_recur,
    )
    return pl.pallas_call(
        copy_out,
        out_shape=jax.ShapeDtypeStruct((OUT, D), BF16),
        in_specs=[anyspec],
        out_specs=anyspec,
        scratch_shapes=[
            pltpu.VMEM((4, OUT // 4, D), BF16), pltpu.SemaphoreType.DMA((4,)), pltpu.SemaphoreType.DMA((4,)),
        ],
    )(full)


def solution(mesh):
    placed = (
        P("sp", None), P(), P(None, "tp"), P(None, "tp"), P(None, "tp"), P(None, "tp"), P(None, "tp"),
        P("tp", None, None), P("tp"), P("tp"), P("sp", "tp"), P("tp"), P("tp", None, None),
        P("tp", None), P("tp", None),
    )
    return jax.shard_map(
        per_device, mesh=mesh, in_specs=placed, out_specs=P(("sp", "tp"), None), check_vma=False
    )
```

```python
import jax
import jax.numpy as jnp
from jax import lax
from jax.experimental import pallas as pl
from jax.experimental.pallas import tpu as pltpu
from jax.sharding import PartitionSpec as P

MESH = pl.DeviceIdType.MESH
F32 = jnp.float32
BF16 = jnp.bfloat16
EPS = 1e-5

ROWS = 1536
OUT = 384
BL = 128
NB = ROWS // BL
C = 256
HK = 128
D = 2048
PF = HK + 16

NT = (((1,), (1,)), ((), ()))
TN = (((0,), (0,)), ((), ()))
NN = (((1,), (0,)), ((), ()))

LOG2E = 1.4426950408889634
POLY = (-LOG2E, -0.7213472908955184, -0.48097089760573397, -0.3571200043786398, -0.3431147843908393)


def dot(a, b, dims=NN):
    return lax.dot_general(a, b, dims, preferred_element_type=F32)


def silu(v):
    half = 0.5 * v
    return half + half * jnp.tanh(half)


def twice(a):
    return jnp.concatenate([a, a], axis=1)


def diag2(a, b):
    zero = jnp.zeros((HK, HK), BF16)
    top = jnp.concatenate([a, zero], axis=1)
    return jnp.concatenate([top, jnp.concatenate([zero, b], axis=1)], axis=0)


def kernel(
    x_hbm, gain_hbm, wp_hbm, wq_hbm, wf_hbm, wv_hbm, wg_hbm, mix_hbm, pscale_hbm, lb_hbm,
    extra_hbm, rgain_hbm, init_hbm, op_hbm, or_hbm,
    out_ref,
    xbuf, xhalo, nbuf, wf, wv, wq, wg, wp, wst, wout, gain, pscale, lb, rgain, extra, mix, init,
    rsbuf, ecum, fbuf, vbuf, ebuf, kdiag, vdiag, qbuf, winbuf, gbuf, pbuf, sloc, run, lrun, vecs,
    totsend, totrecv, ybuf, zbuf, pst, carr, trilb, band,
    ypbuf, ypseen, yrbuf, yrseen, acc, obuf,
    lsem, wsem, w1r, w1fr, w2r, w2fr, w3r,
    es, er, ys, yr_, zs, zr, cs, cr, hs, hr, aps, apr, ars, arr, osem,
):
    x = lax.axis_index("tp")
    sp = lax.axis_index("sp")
    c = lax.rem(sp, 2)
    chip = lax.div(sp, 2)
    y = lax.rem(chip, 4)
    z = lax.div(chip, 4)

    def dev(spi, tpi):
        return {"sp": spi, "tp": tpi}

    def xpeer(k):
        return dev(sp, lax.rem(x + k, 4))

    def ypeer(k):
        return dev(z * 8 + lax.rem(y + k, 4) * 2 + c, x)

    def zpeer(k):
        return dev(lax.rem(z + k, 4) * 8 + y * 2 + c, x)

    sib = dev(sp + 1 - 2 * c, x)
    nxt = dev(lax.rem(sp + 1, 32), x)
    prv = dev(lax.rem(sp + 31, 32), x)

    count = [0]

    def load(src, dst, same=None):
        i = count[0] if same is None else same
        count[0] = max(count[0], i + 1)
        cp = pltpu.make_async_copy(src, dst, lsem.at[i])
        cp.start()
        return cp

    def wait_bytes(ref, sem):
        pltpu.make_async_copy(ref, ref, sem).wait()

    def remote(src, dst, ssem, rsem, to, start=True):
        cp = pltpu.make_async_remote_copy(
            src_ref=src, dst_ref=dst, send_sem=ssem, recv_sem=rsem, device_id=to, device_id_type=MESH
        )
        if start:
            cp.start()
        return cp

    def rows(i, n):
        return pl.ds(pl.multiple_of(i * n, n), n)

    pa = pl.multiple_of(y * 32, 32)
    pb = pl.multiple_of(128 + z * 32, 32)
    l_extra = load(extra_hbm, extra)
    l_gain = load(gain_hbm, gain)
    l_x = [load(x_hbm.at[pl.ds(0, OUT)], xbuf.at[pl.ds(0, OUT)])]
    load(wf_hbm, wf)
    i_wfv = count[0] - 1
    load(wv_hbm, wv, i_wfv)
    l_lb = load(lb_hbm, lb)
    bar = pltpu.get_barrier_semaphore()
    for k in (1, 2, 3):
        for peer in (xpeer, ypeer, zpeer):
            pl.semaphore_signal(bar, inc=1, device_id=peer(k), device_id_type=MESH)
    pl.semaphore_signal(bar, inc=1, device_id=sib, device_id_type=MESH)

    @pl.when(sp < 31)
    def _():
        pl.semaphore_signal(bar, inc=1, device_id=nxt, device_id_type=MESH)

    @pl.when(sp > 0)
    def _():
        pl.semaphore_signal(bar, inc=1, device_id=prv, device_id_type=MESH)


    def extra_sums(b):
        parts = []
        for h in range(2):
            e = extra[h : h + 1, b * BL : (b + 1) * BL] * LOG2E
            hi = e.astype(BF16)
            lo = (e - hi.astype(F32)).astype(BF16)
            t = trilb[...]
            parts.append(jnp.concatenate([t * hi, t * lo], axis=1))
        o = dot(jnp.concatenate(parts, axis=0), jnp.ones((2 * BL, HK), BF16))
        r = pl.ds(b * BL, BL)
        ecum[r, 0:HK] = o[:BL]
        ecum[r, HK:] = o[BL:]

    def norm(j):
        g = gain[...].astype(BF16)
        sums = []
        for s in range(3):
            r = pl.ds(j * OUT + s * BL, BL)
            v = xbuf[r, :]
            nbuf[r, :] = v * g
            sq = v * v
            t = [sq[:, i * 256 : (i + 1) * 256] for i in range(8)]
            while len(t) > 1:
                t = [t[i] + t[i + 1] for i in range(0, len(t), 2)]
            sums.append(t[0])
        ss = dot(jnp.concatenate(sums, axis=0), jnp.ones((256, HK), BF16))
        rsbuf[pl.ds(j * OUT, OUT), :] = lax.rsqrt(ss * (1.0 / D) + EPS)

    def proj_fv(j):
        r = pl.ds(j * OUT, OUT)
        n = nbuf[r, :]
        rs = twice(rsbuf[r, :])
        fbuf[r, :] = dot(n, wf[...]) * (0.5 * rs)
        vbuf[r, :] = (dot(n, wv[...]) * rs).astype(BF16)

    def state_block(b):
        r = pl.ds(b * BL, BL)
        half = 0.5 * (1.0 - lb[...])
        key = half - half * jnp.tanh(fbuf[r, :])
        lf = POLY[4] * key + POLY[3]
        for n in (2, 1, 0):
            lf = lf * key + POLY[n]
        lf = lf * key
        hi = lf.astype(BF16)
        lo = (lf - hi.astype(F32)).astype(BF16)
        t = trilb[...]
        cum = dot(twice(t), jnp.concatenate([hi, lo], axis=0)) + ecum[r, :]
        m = cum[BL // 2 - 1 : BL // 2, :]
        last = cum[BL - 1 : BL, :]
        rel = cum - m
        ebuf[r, :] = jnp.exp2(rel)
        kd = (key * jnp.exp2(-rel)).astype(BF16)
        v = vbuf[r, :]
        for h in range(2):
            hc = slice(h * HK, (h + 1) * HK)
            kdiag[b, hc, hc] = kd[:, hc]
            vdiag[b, hc, hc] = v[:, hc]
        lpre = lrun[...]
        vecs[b, 0:1, :] = lpre
        vecs[b, 1:2, :] = m
        lrun[...] = lpre + last
        a = jnp.exp2(last)
        e2 = jnp.exp2(last - m)
        contrib = dot(v, kd, TN)
        for h in range(2):
            hc = slice(h * HK, (h + 1) * HK)
            s = run[h]
            sloc[b, h] = s
            run[h] = s * a[:, hc] + contrib[hc, hc] * e2[:, hc]

    def proj_p(i):
        r = pl.ds(i * OUT, OUT)
        o = dot(nbuf[r, :], wp[...]) * twice(rsbuf[r, :])
        pbuf[pl.ds(BL + i * OUT, OUT), :] = o.astype(BF16)

    def proj_first():
        v = xhalo[...]
        sq = v * v
        t = [sq[:, i * 256 : (i + 1) * 256] for i in range(8)]
        while len(t) > 1:
            t = [t[i] + t[i + 1] for i in range(0, len(t), 2)]
        ss = dot(t[0], jnp.ones((256, HK), BF16))
        rs = jnp.concatenate([lax.rsqrt(ss * (1.0 / D) + EPS), rsbuf[pl.ds(0, OUT), :]], axis=0)
        n = jnp.concatenate([v * gain[...].astype(BF16), nbuf[pl.ds(0, OUT), :]], axis=0)
        pbuf[pl.ds(BL - 16, OUT + 16), :] = (dot(n, wp[...]) * twice(rs)).astype(BF16)

    def proj_qg(d):
        r = rows(d, OUT)
        n = nbuf[r, :]
        rs = twice(rsbuf[r, :])
        qbuf[r, :] = (silu(dot(n, wq[...]) * rs) * ebuf[r, :]).astype(BF16)
        gbuf[r, :] = silu(dot(n, wg[...]) * rs) * rgain[...]

    def score_block(b):
        r = rows(b, BL)
        s = dot(qbuf[r, :], kdiag[b], NT)
        s = jnp.where(twice(trilb[...]) > 0, s, 0.0).astype(BF16)
        winbuf[r, :] = dot(s, vdiag[b])

    def pool_rows(d):
        parts = []
        for s in range(3):
            b = d * 3 + s
            ext = pbuf[pl.ds(pl.multiple_of(b * BL, BL), 2 * BL), :]
            sums = dot(band[...], ext)
            t = sp * ROWS + b * BL + lax.broadcasted_iota(jnp.int32, (BL, 1), 0)
            cnt = jnp.minimum(t + 1, w).astype(F32)
            parts.append((sums * (1.0 / cnt) - ext[BL:, :].astype(F32)).astype(BF16))
        return (dot(jnp.concatenate(parts, axis=0), mix[0]) * pscale[...]).astype(BF16)

    def out_block(b):
        r = rows(b, BL)
        lpre = vecs[b, 0:1, :]
        m = vecs[b, 1:2, :]
        em = jnp.exp2(m)
        elm = jnp.exp2(lpre + m)
        st = [
            (sloc[b, h] * em[:, h * HK : (h + 1) * HK] + carr[h] * elm[:, h * HK : (h + 1) * HK]).astype(BF16)
            for h in range(2)
        ]
        o = winbuf[r, :] + dot(qbuf[r, :], diag2(st[0], st[1]), NT)
        g = gbuf[r, :]
        parts = []
        for h in range(2):
            hc = slice(h * HK, (h + 1) * HK)
            oh = o[:, hc]
            ms = jnp.sum(oh * oh, axis=-1, keepdims=True) * (1.0 / HK)
            parts.append(oh * lax.rsqrt(ms + EPS) * g[:, hc])
        return jnp.concatenate(parts, axis=1).astype(BF16)

    def chain(ea, eS, la, lS):
        return ea * la, la * eS + lS

    def put_state(ref, a, S):
        hi = a.astype(BF16)
        lo = (a - hi.astype(F32)).astype(BF16)
        ref[0:HK, :] = S.astype(BF16)
        ref[HK : HK + 8, :] = jnp.broadcast_to(hi, (8, HK))
        ref[HK + 8 : HK + 16, :] = jnp.broadcast_to(lo, (8, HK))

    def scan_states(ref, me):
        ta = jnp.ones((1, HK), F32)
        tS = jnp.zeros((HK, HK), F32)
        ea, eS = ta, tS
        for j in range(4):
            full = ref[j].astype(F32)
            ta, tS = chain(ta, tS, full[HK : HK + 1, :] + full[HK + 8 : HK + 9, :], full[0:HK, :])
            ea = jnp.where(me > j, ta, ea)
            eS = jnp.where(me > j, tS, eS)
        return ta, tS, ea, eS


    def shard_of(k):
        return lax.rem(x + 4 - k, 4)

    def piece(k, a, at, half=None):
        start = shard_of(k) * 256 + a * 128 + at * 32
        if half is None:
            return wout.at[c, pl.ds(pl.multiple_of(start, 32), 32)]
        return wout.at[c, pl.ds(pl.multiple_of(start + half * 16, 16), 16)]

    def mine(a):
        return z if a else y

    def w1_send():
        for a in (1, 0):
            for k in (1, 3):
                remote(wst.at[c, a], piece(0, a, mine(a)), wsem, w1r.at[a], xpeer(k))

    def w2_first(k, a):
        for q in (1, 3):
            sl = piece(k, a, mine(a))
            remote(sl, sl, wsem, w2r.at[a, k - 1], (zpeer if a else ypeer)(q))

    def w1_poll(a):
        wait_bytes(nbuf.at[pl.ds(0, 64)], w1r.at[a])
        for h, k in enumerate((1, 3)):
            sl = piece(k, a, mine(a), h)
            remote(sl, sl, wsem, w1fr.at[a], xpeer(k))
            w2_first(k, a)

    def w1_poll2(a):
        wait_bytes(nbuf.at[pl.ds(0, 32)], w1fr.at[a])
        w2_first(2, a)

    def w3_send(k, a, q):
        sl = piece(k, a, lax.rem(mine(a) + q, 4))
        remote(sl, sl, wsem, w3r, sib)

    def w2_poll(k, a):
        wait_bytes(nbuf.at[pl.ds(0, 64)], w2r.at[a, k - 1])
        for h, q in enumerate((1, 3)):
            sl = piece(k, a, lax.rem(mine(a) + 4 - q, 4), h)
            remote(sl, sl, wsem, w2fr.at[a, k - 1], (zpeer if a else ypeer)(q))
        for q in (0, 1, 3):
            w3_send(k, a, q)

    def w3_poll(k, a):
        wait_bytes(nbuf.at[pl.ds(0, 32)], w2fr.at[a, k - 1])
        w3_send(k, a, 2)

    r_i = lax.broadcasted_iota(jnp.int32, (BL, BL), 0)
    c_i = lax.broadcasted_iota(jnp.int32, (BL, BL), 1)
    trilb[...] = jnp.where(c_i <= r_i, 1.0, 0.0).astype(BF16)
    w = lax.shift_left(jnp.int32(2), x)
    r_w = lax.broadcasted_iota(jnp.int32, (BL, 2 * BL), 0)
    c_w = lax.broadcasted_iota(jnp.int32, (BL, 2 * BL), 1)
    diff = r_w + BL - c_w
    band[...] = jnp.where((diff >= 0) & (diff < w), 1.0, 0.0).astype(BF16)
    run[...] = jnp.zeros_like(run)
    lrun[...] = jnp.zeros_like(lrun)
    pbuf[pl.ds(0, BL - 16), :] = jnp.zeros((BL - 16, C), BF16)
    for b in range(NB):
        for h in range(2):
            hc, oc = slice(h * HK, (h + 1) * HK), slice((1 - h) * HK, (2 - h) * HK)
            kdiag[b, hc, oc] = jnp.zeros((HK, HK), BF16)
            vdiag[b, hc, oc] = jnp.zeros((HK, HK), BF16)
    l_extra.wait()
    for b in range(NB):
        extra_sums(b)

    l_gain.wait()
    l_x[0].wait()
    norm(0)
    i_pc = count[0]
    load(op_hbm.at[pl.ds(pa, 32)], wst.at[0, 0], i_pc)
    load(op_hbm.at[pl.ds(pb, 32)], wst.at[0, 1], i_pc)
    load(or_hbm.at[pl.ds(pa, 32)], wst.at[1, 0], i_pc)
    load(or_hbm.at[pl.ds(pb, 32)], wst.at[1, 1], i_pc)
    for i in range(1, 4):
        l_x.append(load(x_hbm.at[pl.ds(i * OUT, OUT)], xbuf.at[pl.ds(i * OUT, OUT)]))
    l_p = load(wp_hbm, wp)
    i_qg = count[0]
    load(wq_hbm, wq, i_qg)
    load(wg_hbm, wg, i_qg)
    l_init = load(init_hbm, init)
    l_rg = load(rgain_hbm, rgain)
    l_ps = load(pscale_hbm, pscale)
    l_mix = load(mix_hbm, mix)
    i_own = count[0]
    load(op_hbm, wout.at[0, rows(x, 256)], i_own)
    load(or_hbm, wout.at[1, rows(x, 256)], i_own)
    wait_bytes(nbuf.at[pl.ds(0, 512)], lsem.at[i_wfv])
    l_lb.wait()
    proj_fv(0)
    wait_bytes(wst, lsem.at[i_pc])
    pl.semaphore_wait(bar, jnp.where((sp == 0) | (sp == 31), 11, 12))
    w1_send()
    h_cp = remote(x_hbm.at[pl.ds(ROWS - 16, 16)], xhalo, hs, hr, nxt, False)

    @pl.when(sp < 31)
    def _():
        h_cp.start()

    l_x[1].wait()
    norm(1)
    l_x[2].wait()
    proj_fv(1)
    norm(2)
    for s in range(3):
        state_block(s)
    l_x[3].wait()
    proj_fv(2)
    norm(3)
    for s in range(3):
        state_block(3 + s)
    proj_fv(3)
    for s in range(3):
        state_block(6 + s)
    for s in range(3):
        state_block(9 + s)

    for h in range(2):
        totsend[h, 0:HK, :] = run[h]
        al = jnp.exp2(lrun[:, h * HK : (h + 1) * HK])
        totsend[h, HK : HK + 8, :] = jnp.broadcast_to(al, (8, HK))
    e_cp = remote(totsend, totrecv, es, er, sib)

    l_p.wait()
    proj_p(3)
    proj_p(2)
    w1_poll(1)
    e_cp.wait()
    oS, oa = totsend[c, 0:HK, :], totsend[c, HK : HK + 1, :]
    sS, sa = totrecv[c, 0:HK, :], totrecv[c, HK : HK + 1, :]
    first = c == 0
    ea, eS = jnp.where(first, oa, sa), jnp.where(first, oS, sS)
    la, lS = jnp.where(first, sa, oa), jnp.where(first, sS, oS)
    put_state(ybuf.at[y], *chain(ea, eS, la, lS))
    for k in (2, 1, 3):
        remote(ybuf.at[y], ybuf.at[y], ys, yr_, ypeer(k))

    @pl.when(sp < 31)
    def _():
        h_cp.wait_send()

    @pl.when(sp > 0)
    def _():
        h_cp.wait_recv()

    proj_p(1)
    proj_first()

    @pl.when(sp == 0)
    def _():
        pbuf[pl.ds(BL - 16, 16), :] = jnp.zeros((16, C), BF16)

    l_ps.wait()
    l_mix.wait()
    w1_poll(0)

    def do_pool(ks):
        blks = [pool_rows(lax.rem(x + k, 4)) for k in ks]
        for k, blk in zip(ks, blks):
            if k:
                ypbuf[k - 1] = blk
            else:
                ypseen[x] = blk
        for k in ks:
            if k:
                remote(ypbuf.at[k - 1], ypseen.at[x], aps, apr, xpeer(k))

    do_pool((1, 3))
    do_pool((2, 0))

    def do_proj(k):
        proj_qg(lax.rem(x + k, 4))

    def do_scores(k):
        for s in range(3):
            score_block(lax.rem(x + k, 4) * 3 + s)

    def do_qg(k):
        do_proj(k)
        do_scores(k)


    def do_out(ks):
        blks = [[out_block(lax.rem(x + k, 4) * 3 + s) for s in range(3)] for k in ks]
        for k, blk in zip(ks, blks):
            for s in range(3):
                if k:
                    yrbuf[k - 1, pl.ds(s * BL, BL), :] = blk[s]
                else:
                    yrseen[x, pl.ds(s * BL, BL), :] = blk[s]
        for k in ks:
            if k:
                remote(yrbuf.at[k - 1], yrseen.at[x], ars, arr.at[k % 2], xpeer(k))

    wait_bytes(nbuf.at[pl.ds(0, 512)], lsem.at[i_qg])
    l_rg.wait()
    do_proj(1)
    wait_bytes(ybuf.at[pl.ds(0, 3)], yr_)
    wait_bytes(ybuf.at[pl.ds(0, 3)], ys)
    ta, tS, ya, yS = scan_states(ybuf, y)
    put_state(zbuf.at[z], ta, tS)
    pst[0:HK, :] = yS
    pst[HK : HK + 8, :] = jnp.broadcast_to(ya, (8, HK))
    z_cp = {
        k: remote(zbuf.at[z], zbuf.at[z], zs.at[k - 1], zr.at[k - 1], zpeer(k), False) for k in (2, 1, 3)
    }
    for k, cp in z_cp.items():
        pl.when(z + k < 4)(cp.start)
    w1_poll2(1)
    do_scores(1)
    w1_poll2(0)
    do_qg(3)
    do_proj(2)
    for k, cp in z_cp.items():
        pl.when(z >= k)(cp.wait_recv)
    ta, tS, za, zS = scan_states(zbuf, z)
    l_init.wait()
    fa, fS = chain(za, zS, pst[HK : HK + 1, :], pst[0:HK, :])
    carr[c] = fa * jnp.transpose(init[c]) + fS
    c_cp = remote(carr.at[c], carr.at[c], cs, cr, sib)
    do_scores(2)
    w2_poll(1, 1)
    w2_poll(1, 0)
    c_cp.wait()
    for h in range(2):
        cur = carr[h]
        later = totrecv[h, HK : HK + 1, :] * cur + totrecv[h, 0:HK, :]
        carr[h] = jnp.where(c == 0, cur, later)
    do_out((1, 3))
    do_out((2,))
    w2_poll(3, 1)
    w2_poll(3, 0)
    w2_poll(2, 1)
    do_proj(0)
    w2_poll(2, 0)
    do_scores(0)
    do_out((0,))
    w3_poll(1, 1)
    w3_poll(1, 0)
    w3_poll(3, 1)
    wait_bytes(nbuf.at[pl.ds(0, 512)], lsem.at[i_own])

    def out_dot(parts, nc):
        left = [(yrseen if mat else ypseen)[shard_of(k)] for mat, k in parts]
        right = [wout[mat, rows(shard_of(k), 256), nc] for mat, k in parts]
        return dot(jnp.concatenate(left, axis=1), jnp.concatenate(right, axis=0))

    for n in range(4):
        nc = pl.ds(n * 512, 512)
        acc[:, nc] = out_dot(((0, 0), (1, 0)), nc)
    w3_poll(3, 0)
    w3_poll(2, 1)
    w3_poll(2, 0)
    wait_bytes(ypbuf, apr)
    wait_bytes(ypbuf, aps)
    wait_bytes(nbuf.at[pl.ds(0, 768)], w3r)
    for n in range(4):
        nc = pl.ds(n * 512, 512)
        acc[:, nc] += out_dot(((0, 1), (0, 3), (0, 2)), nc)
    wait_bytes(yrbuf.at[pl.ds(0, 2)], arr.at[1])
    for n in range(4):
        nc = pl.ds(n * 512, 512)
        acc[:, nc] += out_dot(((1, 1), (1, 3)), nc)
    wait_bytes(yrbuf.at[0], arr.at[0])
    for n in range(4):
        nc = pl.ds(n * 512, 512)
        obuf[n] = (acc[:, nc] + out_dot(((1, 2),), nc)).astype(BF16)
        pltpu.make_async_copy(obuf.at[n], out_ref.at[:, nc], osem).start()
    for k, cp in z_cp.items():
        pl.when(z + k < 4)(cp.wait_send)
    wait_bytes(nbuf, wsem)
    wait_bytes(yrbuf, ars)
    wait_bytes(nbuf.at[pl.ds(0, OUT)], osem)


def copy_out(src, dst, buf, sin, sout):
    n = OUT // 4
    into = [pltpu.make_async_copy(src.at[pl.ds(i * n, n)], buf.at[i], sin.at[i]) for i in range(4)]
    out = [pltpu.make_async_copy(buf.at[i], dst.at[pl.ds(i * n, n)], sout.at[i]) for i in range(4)]
    for cp in into:
        cp.start()
    for cp, to in zip(into, out):
        cp.wait()
        to.start()
    for to in out:
        to.wait()


def scratch():
    V = pltpu.VMEM
    S = pltpu.SemaphoreType.DMA
    return [
        V((ROWS, D), BF16), V((16, D), BF16), V((ROWS, D), BF16), V((D, C), BF16), V((D, C), BF16), V((D, C), BF16),
        V((D, C), BF16), V((D, C), BF16),         V((2, 2, 32, D), BF16), V((2, 4 * C, D), BF16),
        V((1, D), F32), V((1, C), F32), V((1, C), F32), V((1, C), F32),
        V((2, ROWS), F32), V((1, C, C), BF16), V((2, HK, HK), F32),
        V((ROWS, HK), F32), V((ROWS, C), F32), V((ROWS, C), F32), V((ROWS, C), BF16), V((ROWS, C), F32),
        V((NB, C, C), BF16), V((NB, C, C), BF16), V((ROWS, C), BF16), V((ROWS, C), F32), V((ROWS, C), F32),
        V((BL + ROWS, C), BF16), V((NB, 2, HK, HK), F32), V((2, HK, HK), F32), V((1, C), F32), V((NB, 2, C), F32),
        V((2, HK + 8, HK), F32), V((2, HK + 8, HK), F32), V((4, PF, HK), BF16), V((4, PF, HK), BF16), V((HK + 8, HK), F32), V((2, HK, HK), F32),
        V((BL, BL), BF16), V((BL, 2 * BL), BF16),
        V((3, OUT, C), BF16), V((4, OUT, C), BF16), V((3, OUT, C), BF16), V((4, OUT, C), BF16),
        V((OUT, D), F32), V((4, OUT, 512), BF16),
        S((17,)), S(()), S((2,)), S((2,)), S((2, 3)), S((2, 3)), S(()),
        S(()), S(()), S(()), S(()), S((3,)), S((3,)), S(()), S(()), S(()), S(()), S(()), S(()), S(()), S((2,)), S(()),
    ]


def per_device(
    inputs, norm_gain, pool_weight, query_weight, forget_weight, value_weight, outgate_weight,
    pool_mix, pool_scale, lower_bound, extra_decay, recur_gain, init_state, out_pool, out_recur,
):
    anyspec = pl.BlockSpec(memory_space=pl.ANY)
    full = pl.pallas_call(
        kernel,
        out_shape=jax.ShapeDtypeStruct((OUT, D), BF16),
        in_specs=[anyspec] * 15,
        out_specs=anyspec,
        scratch_shapes=scratch(),
        compiler_params=pltpu.CompilerParams(
            collective_id=0, has_side_effects=True, vmem_limit_bytes=63 * 1024 * 1024
        ),
    )(
        inputs, norm_gain.reshape(1, D), pool_weight, query_weight, forget_weight, value_weight,
        outgate_weight, pool_mix, pool_scale.reshape(1, C), lower_bound.reshape(1, C),
        extra_decay.T, recur_gain.reshape(1, C), init_state, out_pool, out_recur,
    )
    return pl.pallas_call(
        copy_out,
        out_shape=jax.ShapeDtypeStruct((OUT, D), BF16),
        in_specs=[anyspec],
        out_specs=anyspec,
        scratch_shapes=[
            pltpu.VMEM((4, OUT // 4, D), BF16), pltpu.SemaphoreType.DMA((4,)), pltpu.SemaphoreType.DMA((4,)),
        ],
    )(full)


def solution(mesh):
    placed = (
        P("sp", None), P(), P(None, "tp"), P(None, "tp"), P(None, "tp"), P(None, "tp"), P(None, "tp"),
        P("tp", None, None), P("tp"), P("tp"), P("sp", "tp"), P("tp"), P("tp", None, None),
        P("tp", None), P("tp", None),
    )
    return jax.shard_map(
        per_device, mesh=mesh, in_specs=placed, out_specs=P(("sp", "tp"), None), check_vma=False
    )
```

```python
import jax
import jax.numpy as jnp
from jax import lax
from jax.experimental import pallas as pl
from jax.experimental.pallas import tpu as pltpu
from jax.sharding import PartitionSpec as P

MESH = pl.DeviceIdType.MESH
F32 = jnp.float32
BF16 = jnp.bfloat16
EPS = 1e-5

ROWS = 1536
OUT = 384
BL = 128
NB = ROWS // BL
C = 256
HK = 128
D = 2048
PF = HK + 16

NT = (((1,), (1,)), ((), ()))
TN = (((0,), (0,)), ((), ()))
NN = (((1,), (0,)), ((), ()))

LOG2E = 1.4426950408889634
POLY = (-LOG2E, -0.7213472908955184, -0.48097089760573397, -0.3571200043786398, -0.3431147843908393)


def dot(a, b, dims=NN):
    return lax.dot_general(a, b, dims, preferred_element_type=F32)


def silu(v):
    half = 0.5 * v
    return half + half * jnp.tanh(half)


def twice(a):
    return jnp.concatenate([a, a], axis=1)


def diag2(a, b):
    zero = jnp.zeros((HK, HK), BF16)
    top = jnp.concatenate([a, zero], axis=1)
    return jnp.concatenate([top, jnp.concatenate([zero, b], axis=1)], axis=0)


def kernel(
    x_hbm, gain_hbm, wp_hbm, wq_hbm, wf_hbm, wv_hbm, wg_hbm, mix_hbm, pscale_hbm, lb_hbm,
    extra_hbm, rgain_hbm, init_hbm, op_hbm, or_hbm,
    out_ref,
    xbuf, xhalo, nbuf, wf, wv, wq, wg, wp, wst, wout, gain, pscale, lb, rgain, extra, mix, init,
    rsbuf, ecum, fbuf, vbuf, ebuf, kdiag, vdiag, qbuf, winbuf, gbuf, pbuf, sloc, run, lrun, vecs,
    totsend, totrecv, ybuf, zbuf, pst, carr, trilb, band,
    ypbuf, ypseen, yrbuf, yrseen, acc, obuf,
    lsem, wsem, w1r, w1fr, w2r, w2fr, w3r,
    es, er, yr_, zs, zr, cr, hs, hr, aps, apr, ars, arr, osem,
):
    x = lax.axis_index("tp")
    sp = lax.axis_index("sp")
    c = lax.rem(sp, 2)
    chip = lax.div(sp, 2)
    y = lax.rem(chip, 4)
    z = lax.div(chip, 4)

    def dev(spi, tpi):
        return {"sp": spi, "tp": tpi}

    def xpeer(k):
        return dev(sp, lax.rem(x + k, 4))

    def ypeer(k):
        return dev(z * 8 + lax.rem(y + k, 4) * 2 + c, x)

    def zpeer(k):
        return dev(lax.rem(z + k, 4) * 8 + y * 2 + c, x)

    sib = dev(sp + 1 - 2 * c, x)
    nxt = dev(lax.rem(sp + 1, 32), x)
    prv = dev(lax.rem(sp + 31, 32), x)

    count = [0]

    def load(src, dst, same=None):
        i = count[0] if same is None else same
        count[0] = max(count[0], i + 1)
        cp = pltpu.make_async_copy(src, dst, lsem.at[i])
        cp.start()
        return cp

    def wait_bytes(ref, sem):
        pltpu.make_async_copy(ref, ref, sem).wait()

    def remote(src, dst, ssem, rsem, to, start=True):
        cp = pltpu.make_async_remote_copy(
            src_ref=src, dst_ref=dst, send_sem=ssem, recv_sem=rsem, device_id=to, device_id_type=MESH
        )
        if start:
            cp.start()
        return cp

    def rows(i, n):
        return pl.ds(pl.multiple_of(i * n, n), n)

    pa = pl.multiple_of(y * 32, 32)
    pb = pl.multiple_of(128 + z * 32, 32)
    l_extra = load(extra_hbm, extra)
    l_gain = load(gain_hbm, gain)
    l_x = [load(x_hbm.at[pl.ds(0, OUT)], xbuf.at[pl.ds(0, OUT)])]
    load(wf_hbm, wf)
    i_wfv = count[0] - 1
    load(wv_hbm, wv, i_wfv)
    l_lb = load(lb_hbm, lb)
    bar = pltpu.get_barrier_semaphore()
    for k in (1, 2, 3):
        for peer in (xpeer, ypeer, zpeer):
            pl.semaphore_signal(bar, inc=1, device_id=peer(k), device_id_type=MESH)
    pl.semaphore_signal(bar, inc=1, device_id=sib, device_id_type=MESH)

    @pl.when(sp < 31)
    def _():
        pl.semaphore_signal(bar, inc=1, device_id=nxt, device_id_type=MESH)

    @pl.when(sp > 0)
    def _():
        pl.semaphore_signal(bar, inc=1, device_id=prv, device_id_type=MESH)


    def extra_sums(b):
        parts = []
        for h in range(2):
            e = extra[h : h + 1, b * BL : (b + 1) * BL] * LOG2E
            hi = e.astype(BF16)
            lo = (e - hi.astype(F32)).astype(BF16)
            t = trilb[...]
            parts.append(jnp.concatenate([t * hi, t * lo], axis=1))
        o = dot(jnp.concatenate(parts, axis=0), jnp.ones((2 * BL, HK), BF16))
        r = pl.ds(b * BL, BL)
        ecum[r, 0:HK] = o[:BL]
        ecum[r, HK:] = o[BL:]

    def norm(j):
        g = gain[...].astype(BF16)
        sums = []
        for s in range(3):
            r = pl.ds(j * OUT + s * BL, BL)
            v = xbuf[r, :]
            nbuf[r, :] = v * g
            sq = v * v
            t = [sq[:, i * 256 : (i + 1) * 256] for i in range(8)]
            while len(t) > 1:
                t = [t[i] + t[i + 1] for i in range(0, len(t), 2)]
            sums.append(t[0])
        ss = dot(jnp.concatenate(sums, axis=0), jnp.ones((256, HK), BF16))
        rsbuf[pl.ds(j * OUT, OUT), :] = lax.rsqrt(ss * (1.0 / D) + EPS)

    def proj_fv(j):
        r = pl.ds(j * OUT, OUT)
        n = nbuf[r, :]
        rs = twice(rsbuf[r, :])
        fbuf[r, :] = dot(n, wf[...]) * (0.5 * rs)
        vbuf[r, :] = (dot(n, wv[...]) * rs).astype(BF16)

    def state_block(b):
        r = pl.ds(b * BL, BL)
        half = 0.5 * (1.0 - lb[...])
        key = half - half * jnp.tanh(fbuf[r, :])
        lf = POLY[4] * key + POLY[3]
        for n in (2, 1, 0):
            lf = lf * key + POLY[n]
        lf = lf * key
        hi = lf.astype(BF16)
        lo = (lf - hi.astype(F32)).astype(BF16)
        t = trilb[...]
        cum = dot(twice(t), jnp.concatenate([hi, lo], axis=0)) + ecum[r, :]
        m = cum[BL // 2 - 1 : BL // 2, :]
        last = cum[BL - 1 : BL, :]
        rel = cum - m
        ebuf[r, :] = jnp.exp2(rel)
        kd = (key * jnp.exp2(-rel)).astype(BF16)
        v = vbuf[r, :]
        for h in range(2):
            hc = slice(h * HK, (h + 1) * HK)
            kdiag[b, hc, hc] = kd[:, hc]
            vdiag[b, hc, hc] = v[:, hc]
        lpre = lrun[...]
        vecs[b, 0:1, :] = lpre
        vecs[b, 1:2, :] = m
        lrun[...] = lpre + last
        a = jnp.exp2(last)
        e2 = jnp.exp2(last - m)
        contrib = dot(v, kd, TN)
        for h in range(2):
            hc = slice(h * HK, (h + 1) * HK)
            s = run[h]
            sloc[b, h] = s
            run[h] = s * a[:, hc] + contrib[hc, hc] * e2[:, hc]

    def proj_p(i):
        r = pl.ds(i * OUT, OUT)
        o = dot(nbuf[r, :], wp[...]) * twice(rsbuf[r, :])
        pbuf[pl.ds(BL + i * OUT, OUT), :] = o.astype(BF16)

    def proj_first():
        v = xhalo[...]
        sq = v * v
        t = [sq[:, i * 256 : (i + 1) * 256] for i in range(8)]
        while len(t) > 1:
            t = [t[i] + t[i + 1] for i in range(0, len(t), 2)]
        ss = dot(t[0], jnp.ones((256, HK), BF16))
        rs = jnp.concatenate([lax.rsqrt(ss * (1.0 / D) + EPS), rsbuf[pl.ds(0, OUT), :]], axis=0)
        n = jnp.concatenate([v * gain[...].astype(BF16), nbuf[pl.ds(0, OUT), :]], axis=0)
        pbuf[pl.ds(BL - 16, OUT + 16), :] = (dot(n, wp[...]) * twice(rs)).astype(BF16)

    def proj_qg(d):
        r = rows(d, OUT)
        n = nbuf[r, :]
        rs = twice(rsbuf[r, :])
        qbuf[r, :] = (silu(dot(n, wq[...]) * rs) * ebuf[r, :]).astype(BF16)
        gbuf[r, :] = silu(dot(n, wg[...]) * rs) * rgain[...]

    def score_block(b):
        r = rows(b, BL)
        s = dot(qbuf[r, :], kdiag[b], NT)
        s = jnp.where(twice(trilb[...]) > 0, s, 0.0).astype(BF16)
        winbuf[r, :] = dot(s, vdiag[b])

    def pool_rows(d):
        parts = []
        for s in range(3):
            b = d * 3 + s
            ext = pbuf[pl.ds(pl.multiple_of(b * BL, BL), 2 * BL), :]
            sums = dot(band[...], ext)
            t = sp * ROWS + b * BL + lax.broadcasted_iota(jnp.int32, (BL, 1), 0)
            cnt = jnp.minimum(t + 1, w).astype(F32)
            parts.append((sums * (1.0 / cnt) - ext[BL:, :].astype(F32)).astype(BF16))
        return (dot(jnp.concatenate(parts, axis=0), mix[0]) * pscale[...]).astype(BF16)

    def out_block(b):
        r = rows(b, BL)
        lpre = vecs[b, 0:1, :]
        m = vecs[b, 1:2, :]
        em = jnp.exp2(m)
        elm = jnp.exp2(lpre + m)
        st = [
            (sloc[b, h] * em[:, h * HK : (h + 1) * HK] + carr[h] * elm[:, h * HK : (h + 1) * HK]).astype(BF16)
            for h in range(2)
        ]
        o = winbuf[r, :] + dot(qbuf[r, :], diag2(st[0], st[1]), NT)
        g = gbuf[r, :]
        parts = []
        for h in range(2):
            hc = slice(h * HK, (h + 1) * HK)
            oh = o[:, hc]
            ms = jnp.sum(oh * oh, axis=-1, keepdims=True) * (1.0 / HK)
            parts.append(oh * lax.rsqrt(ms + EPS) * g[:, hc])
        return jnp.concatenate(parts, axis=1).astype(BF16)

    def chain(ea, eS, la, lS):
        return ea * la, la * eS + lS

    def put_state(ref, a, S):
        hi = a.astype(BF16)
        lo = (a - hi.astype(F32)).astype(BF16)
        ref[0:HK, :] = S.astype(BF16)
        ref[HK : HK + 8, :] = jnp.broadcast_to(hi, (8, HK))
        ref[HK + 8 : HK + 16, :] = jnp.broadcast_to(lo, (8, HK))

    def scan_states(ref, me):
        ta = jnp.ones((1, HK), F32)
        tS = jnp.zeros((HK, HK), F32)
        ea, eS = ta, tS
        for j in range(4):
            full = ref[j].astype(F32)
            ta, tS = chain(ta, tS, full[HK : HK + 1, :] + full[HK + 8 : HK + 9, :], full[0:HK, :])
            ea = jnp.where(me > j, ta, ea)
            eS = jnp.where(me > j, tS, eS)
        return ta, tS, ea, eS


    def shard_of(k):
        return lax.rem(x + 4 - k, 4)

    def piece(k, a, at, half=None):
        start = shard_of(k) * 256 + a * 128 + at * 32
        if half is None:
            return wout.at[c, pl.ds(pl.multiple_of(start, 32), 32)]
        return wout.at[c, pl.ds(pl.multiple_of(start + half * 16, 16), 16)]

    def mine(a):
        return z if a else y

    def w1_send():
        for a in (1, 0):
            for k in (1, 3):
                remote(wst.at[c, a], piece(0, a, mine(a)), wsem, w1r.at[a], xpeer(k))

    def w2_first(k, a):
        for q in (1, 3):
            sl = piece(k, a, mine(a))
            remote(sl, sl, wsem, w2r.at[a, k - 1], (zpeer if a else ypeer)(q))

    def w1_poll(a):
        wait_bytes(nbuf.at[pl.ds(0, 64)], w1r.at[a])
        for h, k in enumerate((1, 3)):
            sl = piece(k, a, mine(a), h)
            remote(sl, sl, wsem, w1fr.at[a], xpeer(k))
            w2_first(k, a)

    def w1_poll2(a):
        wait_bytes(nbuf.at[pl.ds(0, 32)], w1fr.at[a])
        w2_first(2, a)

    def w3_send(k, a, q):
        sl = piece(k, a, lax.rem(mine(a) + q, 4))
        remote(sl, sl, wsem, w3r, sib)

    def w2_poll(k, a):
        wait_bytes(nbuf.at[pl.ds(0, 64)], w2r.at[a, k - 1])
        for h, q in enumerate((1, 3)):
            sl = piece(k, a, lax.rem(mine(a) + 4 - q, 4), h)
            remote(sl, sl, wsem, w2fr.at[a, k - 1], (zpeer if a else ypeer)(q))
        for q in (0, 1, 3):
            w3_send(k, a, q)

    def w3_poll(k, a):
        wait_bytes(nbuf.at[pl.ds(0, 32)], w2fr.at[a, k - 1])
        w3_send(k, a, 2)

    r_i = lax.broadcasted_iota(jnp.int32, (BL, BL), 0)
    c_i = lax.broadcasted_iota(jnp.int32, (BL, BL), 1)
    trilb[...] = jnp.where(c_i <= r_i, 1.0, 0.0).astype(BF16)
    w = lax.shift_left(jnp.int32(2), x)
    r_w = lax.broadcasted_iota(jnp.int32, (BL, 2 * BL), 0)
    c_w = lax.broadcasted_iota(jnp.int32, (BL, 2 * BL), 1)
    diff = r_w + BL - c_w
    band[...] = jnp.where((diff >= 0) & (diff < w), 1.0, 0.0).astype(BF16)
    run[...] = jnp.zeros_like(run)
    lrun[...] = jnp.zeros_like(lrun)
    pbuf[pl.ds(0, BL - 16), :] = jnp.zeros((BL - 16, C), BF16)
    for b in range(NB):
        for h in range(2):
            hc, oc = slice(h * HK, (h + 1) * HK), slice((1 - h) * HK, (2 - h) * HK)
            kdiag[b, hc, oc] = jnp.zeros((HK, HK), BF16)
            vdiag[b, hc, oc] = jnp.zeros((HK, HK), BF16)
    l_extra.wait()
    for b in range(NB):
        extra_sums(b)

    l_gain.wait()
    l_x[0].wait()
    norm(0)
    i_pc = count[0]
    load(op_hbm.at[pl.ds(pa, 32)], wst.at[0, 0], i_pc)
    load(op_hbm.at[pl.ds(pb, 32)], wst.at[0, 1], i_pc)
    load(or_hbm.at[pl.ds(pa, 32)], wst.at[1, 0], i_pc)
    load(or_hbm.at[pl.ds(pb, 32)], wst.at[1, 1], i_pc)
    for i in range(1, 4):
        l_x.append(load(x_hbm.at[pl.ds(i * OUT, OUT)], xbuf.at[pl.ds(i * OUT, OUT)]))
    l_p = load(wp_hbm, wp)
    i_qg = count[0]
    load(wq_hbm, wq, i_qg)
    load(wg_hbm, wg, i_qg)
    l_init = load(init_hbm, init)
    l_rg = load(rgain_hbm, rgain)
    l_ps = load(pscale_hbm, pscale)
    l_mix = load(mix_hbm, mix)
    i_own = count[0]
    load(op_hbm, wout.at[0, rows(x, 256)], i_own)
    load(or_hbm, wout.at[1, rows(x, 256)], i_own)
    wait_bytes(nbuf.at[pl.ds(0, 512)], lsem.at[i_wfv])
    l_lb.wait()
    proj_fv(0)
    wait_bytes(wst, lsem.at[i_pc])
    pl.semaphore_wait(bar, jnp.where((sp == 0) | (sp == 31), 11, 12))
    w1_send()
    h_cp = remote(x_hbm.at[pl.ds(ROWS - 16, 16)], xhalo, hs, hr, nxt, False)

    @pl.when(sp < 31)
    def _():
        h_cp.start()

    l_x[1].wait()
    norm(1)
    l_x[2].wait()
    proj_fv(1)
    norm(2)
    for s in range(3):
        state_block(s)
    l_x[3].wait()
    proj_fv(2)
    norm(3)
    for s in range(3):
        state_block(3 + s)
    proj_fv(3)
    for s in range(3):
        state_block(6 + s)
    for s in range(3):
        state_block(9 + s)

    for h in range(2):
        totsend[h, 0:HK, :] = run[h]
        al = jnp.exp2(lrun[:, h * HK : (h + 1) * HK])
        totsend[h, HK : HK + 8, :] = jnp.broadcast_to(al, (8, HK))
    e_cp = remote(totsend, totrecv, es, er, sib)

    l_p.wait()
    proj_p(3)
    proj_p(2)
    w1_poll(1)
    e_cp.wait()
    oS, oa = totsend[c, 0:HK, :], totsend[c, HK : HK + 1, :]
    sS, sa = totrecv[c, 0:HK, :], totrecv[c, HK : HK + 1, :]
    first = c == 0
    ea, eS = jnp.where(first, oa, sa), jnp.where(first, oS, sS)
    la, lS = jnp.where(first, sa, oa), jnp.where(first, sS, oS)
    put_state(ybuf.at[y], *chain(ea, eS, la, lS))
    for k in (2, 1, 3):
        remote(ybuf.at[y], ybuf.at[y], es, yr_, ypeer(k))

    @pl.when(sp < 31)
    def _():
        h_cp.wait_send()

    @pl.when(sp > 0)
    def _():
        h_cp.wait_recv()

    proj_p(1)
    proj_first()

    @pl.when(sp == 0)
    def _():
        pbuf[pl.ds(BL - 16, 16), :] = jnp.zeros((16, C), BF16)

    l_ps.wait()
    l_mix.wait()
    w1_poll(0)

    def do_pool(ks):
        blks = [pool_rows(lax.rem(x + k, 4)) for k in ks]
        for k, blk in zip(ks, blks):
            if k:
                ypbuf[k - 1] = blk
            else:
                ypseen[x] = blk
        for k in ks:
            if k:
                remote(ypbuf.at[k - 1], ypseen.at[x], aps, apr, xpeer(k))

    do_pool((1, 3))
    do_pool((2, 0))

    def do_proj(k):
        proj_qg(lax.rem(x + k, 4))

    def do_scores(k):
        for s in range(3):
            score_block(lax.rem(x + k, 4) * 3 + s)

    def do_qg(k):
        do_proj(k)
        do_scores(k)


    def do_out(ks):
        blks = [[out_block(lax.rem(x + k, 4) * 3 + s) for s in range(3)] for k in ks]
        for k, blk in zip(ks, blks):
            for s in range(3):
                if k:
                    yrbuf[k - 1, pl.ds(s * BL, BL), :] = blk[s]
                else:
                    yrseen[x, pl.ds(s * BL, BL), :] = blk[s]
        for k in ks:
            if k:
                remote(yrbuf.at[k - 1], yrseen.at[x], ars, arr.at[k % 2], xpeer(k))

    wait_bytes(nbuf.at[pl.ds(0, 512)], lsem.at[i_qg])
    l_rg.wait()
    do_proj(1)
    wait_bytes(ybuf.at[pl.ds(0, 3)], yr_)
    wait_bytes(ybuf.at[pl.ds(0, 3)], es)
    ta, tS, ya, yS = scan_states(ybuf, y)
    put_state(zbuf.at[z], ta, tS)
    pst[0:HK, :] = yS
    pst[HK : HK + 8, :] = jnp.broadcast_to(ya, (8, HK))
    z_cp = {
        k: remote(zbuf.at[z], zbuf.at[z], zs.at[k - 1], zr.at[k - 1], zpeer(k), False) for k in (2, 1, 3)
    }
    for k, cp in z_cp.items():
        pl.when(z + k < 4)(cp.start)
    w1_poll2(1)
    do_scores(1)
    w1_poll2(0)
    do_qg(3)
    do_proj(2)
    for k, cp in z_cp.items():
        pl.when(z >= k)(cp.wait_recv)
    ta, tS, za, zS = scan_states(zbuf, z)
    l_init.wait()
    fa, fS = chain(za, zS, pst[HK : HK + 1, :], pst[0:HK, :])
    carr[c] = fa * jnp.transpose(init[c]) + fS
    c_cp = remote(carr.at[c], carr.at[c], es, cr, sib)
    do_scores(2)
    w2_poll(1, 1)
    w2_poll(1, 0)
    c_cp.wait()
    for h in range(2):
        cur = carr[h]
        later = totrecv[h, HK : HK + 1, :] * cur + totrecv[h, 0:HK, :]
        carr[h] = jnp.where(c == 0, cur, later)
    do_out((1, 3))
    do_out((2,))
    w2_poll(3, 1)
    w2_poll(3, 0)
    w2_poll(2, 1)
    do_proj(0)
    w2_poll(2, 0)
    do_scores(0)
    do_out((0,))
    w3_poll(1, 1)
    w3_poll(1, 0)
    w3_poll(3, 1)
    wait_bytes(nbuf.at[pl.ds(0, 512)], lsem.at[i_own])

    def out_dot(parts, nc):
        left = [(yrseen if mat else ypseen)[shard_of(k)] for mat, k in parts]
        right = [wout[mat, rows(shard_of(k), 256), nc] for mat, k in parts]
        return dot(jnp.concatenate(left, axis=1), jnp.concatenate(right, axis=0))

    for n in range(4):
        nc = pl.ds(n * 512, 512)
        acc[:, nc] = out_dot(((0, 0), (1, 0)), nc)
    w3_poll(3, 0)
    w3_poll(2, 1)
    w3_poll(2, 0)
    wait_bytes(ypbuf, apr)
    wait_bytes(ypbuf, aps)
    wait_bytes(nbuf.at[pl.ds(0, 768)], w3r)
    for n in range(4):
        nc = pl.ds(n * 512, 512)
        acc[:, nc] += out_dot(((0, 1), (0, 3), (0, 2)), nc)
    wait_bytes(yrbuf.at[pl.ds(0, 2)], arr.at[1])
    for n in range(4):
        nc = pl.ds(n * 512, 512)
        acc[:, nc] += out_dot(((1, 1), (1, 3)), nc)
    wait_bytes(yrbuf.at[0], arr.at[0])
    for n in range(4):
        nc = pl.ds(n * 512, 512)
        obuf[n] = (acc[:, nc] + out_dot(((1, 2),), nc)).astype(BF16)
        pltpu.make_async_copy(obuf.at[n], out_ref.at[:, nc], osem).start()
    for k, cp in z_cp.items():
        pl.when(z + k < 4)(cp.wait_send)
    wait_bytes(nbuf, wsem)
    wait_bytes(yrbuf, ars)
    wait_bytes(nbuf.at[pl.ds(0, OUT)], osem)


def copy_out(src, dst, buf, sin, sout):
    n = OUT // 3
    into = [pltpu.make_async_copy(src.at[pl.ds(i * n, n)], buf.at[pl.ds(i * n, n)], sin.at[i]) for i in range(3)]
    for cp in into:
        cp.start()
    for i, cp in enumerate(into):
        cp.wait()
        pltpu.make_async_copy(buf.at[pl.ds(i * n, n)], dst.at[pl.ds(i * n, n)], sout).start()
    pltpu.make_async_copy(buf, dst, sout).wait()


def scratch():
    V = pltpu.VMEM
    S = pltpu.SemaphoreType.DMA
    return [
        V((ROWS, D), BF16), V((16, D), BF16), V((ROWS, D), BF16), V((D, C), BF16), V((D, C), BF16), V((D, C), BF16),
        V((D, C), BF16), V((D, C), BF16),         V((2, 2, 32, D), BF16), V((2, 4 * C, D), BF16),
        V((1, D), F32), V((1, C), F32), V((1, C), F32), V((1, C), F32),
        V((2, ROWS), F32), V((1, C, C), BF16), V((2, HK, HK), F32),
        V((ROWS, HK), F32), V((ROWS, C), F32), V((ROWS, C), F32), V((ROWS, C), BF16), V((ROWS, C), F32),
        V((NB, C, C), BF16), V((NB, C, C), BF16), V((ROWS, C), BF16), V((ROWS, C), F32), V((ROWS, C), F32),
        V((BL + ROWS, C), BF16), V((NB, 2, HK, HK), F32), V((2, HK, HK), F32), V((1, C), F32), V((NB, 2, C), F32),
        V((2, HK + 8, HK), F32), V((2, HK + 8, HK), F32), V((4, PF, HK), BF16), V((4, PF, HK), BF16), V((HK + 8, HK), F32), V((2, HK, HK), F32),
        V((BL, BL), BF16), V((BL, 2 * BL), BF16),
        V((3, OUT, C), BF16), V((4, OUT, C), BF16), V((3, OUT, C), BF16), V((4, OUT, C), BF16),
        V((OUT, D), F32), V((4, OUT, 512), BF16),
        S((16,)), S(()), S((2,)), S((2,)), S((2, 3)), S((2, 3)), S(()),
        S(()), S(()), S(()), S((3,)), S((3,)), S(()), S(()), S(()), S(()), S(()), S(()), S((2,)), S(()),
    ]


def per_device(
    inputs, norm_gain, pool_weight, query_weight, forget_weight, value_weight, outgate_weight,
    pool_mix, pool_scale, lower_bound, extra_decay, recur_gain, init_state, out_pool, out_recur,
):
    anyspec = pl.BlockSpec(memory_space=pl.ANY)
    full = pl.pallas_call(
        kernel,
        out_shape=jax.ShapeDtypeStruct((OUT, D), BF16),
        in_specs=[anyspec] * 15,
        out_specs=anyspec,
        scratch_shapes=scratch(),
        compiler_params=pltpu.CompilerParams(
            collective_id=0, has_side_effects=True, vmem_limit_bytes=63 * 1024 * 1024
        ),
    )(
        inputs, norm_gain.reshape(1, D), pool_weight, query_weight, forget_weight, value_weight,
        outgate_weight, pool_mix, pool_scale.reshape(1, C), lower_bound.reshape(1, C),
        extra_decay.T, recur_gain.reshape(1, C), init_state, out_pool, out_recur,
    )
    return pl.pallas_call(
        copy_out,
        out_shape=jax.ShapeDtypeStruct((OUT, D), BF16),
        in_specs=[anyspec],
        out_specs=anyspec,
        scratch_shapes=[
            pltpu.VMEM((OUT, D), BF16), pltpu.SemaphoreType.DMA((3,)), pltpu.SemaphoreType.DMA(()),
        ],
    )(full)


def solution(mesh):
    placed = (
        P("sp", None), P(), P(None, "tp"), P(None, "tp"), P(None, "tp"), P(None, "tp"), P(None, "tp"),
        P("tp", None, None), P("tp"), P("tp"), P("sp", "tp"), P("tp"), P("tp", None, None),
        P("tp", None), P("tp", None),
    )
    return jax.shard_map(
        per_device, mesh=mesh, in_specs=placed, out_specs=P(("sp", "tp"), None), check_vma=False
    )
```
